512 devices in a mesh: grp: 2 (over y), sp: 32 (over z), tp: 8 (over x, core).
Axes of the slice: x: 4, y: 2, z: 32, core: 2. Of those that a mesh axis runs over, the one named last changes fastest.
The devices are a block of a 4x8x32 slice.
Arguments:
- window_query: bfloat16 [20480, 2048], P(('grp', 'sp'), 'tp'), parts along dimension 0, may hold values from -24 to 24
- window_key: bfloat16 [20480, 1024], P(('grp', 'sp'), 'tp'), parts along dimension 0, may hold values from -24 to 24
- window_value: bfloat16 [20480, 1024], P(('grp', 'sp'), 'tp'), parts along dimension 0, may hold values from -6 to 6
- grid_query: bfloat16 [20480, 2048], P(('grp', 'sp'), 'tp'), parts along dimension 0, may hold values from -10 to 10
- grid_key: bfloat16 [20480, 1024], P(('grp', 'sp'), 'tp'), parts along dimension 0, may hold values from -10 to 10
- grid_value: bfloat16 [20480, 1024], P(('grp', 'sp'), 'tp'), parts along dimension 0, may hold values from -6 to 6
- sink_logit: float32 [16], P('tp'), may hold values from 1 to 6
- query_gain: float32 [128], replicated, may hold values from 0.8 to 6
- key_gain: float32 [128], replicated, may hold values from 0.8 to 6
- window_weights: bfloat16 [2048, 4096], P('tp'), may hold values from -0.59765625 to 0.59765625
- grid_weights: bfloat16 [2048, 4096], P('tp'), may hold values from -0.59765625 to 0.59765625
Outputs:
- merged: bfloat16 [20480, 4096], P(('grp', 'sp', 'tp')), parts along dimension 0
The draws below stay inside these ranges and needn't reach their ends.
There are 2 independent parts, one for each index of `grp`. The reference program is written for one: setup_inputs(seed, part) draws one part's arguments, and reference() takes and returns one part's arrays. A program takes and returns all parts, laid end to end along the dimension named above; an argument that names none is the same for every part. Nothing has to cross between parts.
All inputs are finite; a program needn't handle non-finite values.
Results may differ from the reference program's by a relative error of at most 0.014.
The reference program's roundings to bfloat16 on the way count: a program that leaves them out, or rounds other values in their place, can miss the bound.
Values may be sent and summed in bfloat16 or wider, within the bound.
No kernel may reach another device: no remote copies, remote signals or barrier semaphores. Data moves between devices by JAX's collectives and lax.ppermute only.
A program may use at most 64 MiB of HBM per device.

```python
import jax
import jax.numpy as jnp
from jax import lax

D = 4096
HEAD = 128
QH_A = 16
KVH_A = 8
QH_B = 16
KVH_B = 8
WINDOW = 128
GRID_W = 64
TOKENS = 10240
N_SP = 32
N_TP = 8


def pair_window(key):
    base = jax.random.fold_in(key, 101)
    key_query, key_key = jax.random.split(base, 2)
    queries = jnp.clip(jax.random.normal(key_query, (TOKENS, QH_A * HEAD), jnp.float32), -6.0, 6.0)
    keys = jnp.clip(jax.random.normal(key_key, (TOKENS, KVH_A * HEAD), jnp.float32), -6.0, 6.0)
    return (queries, keys)


def pair_grid(key):
    base = jax.random.fold_in(key, 202)
    key_query, key_key = jax.random.split(base, 2)
    queries = jnp.clip(jax.random.normal(key_query, (TOKENS, QH_B * HEAD), jnp.float32), -6.0, 6.0)
    keys = jnp.clip(jax.random.normal(key_key, (TOKENS, KVH_B * HEAD), jnp.float32), -6.0, 6.0)
    return (queries, keys)


def grid_gain(key, salt):
    base = jax.random.fold_in(key, salt)
    return 1.5 + 0.27 * jnp.clip(jax.random.normal(base, (HEAD,), jnp.float32), -2.5, 2.5)


def draw_window_query(key, part):
    return pair_window(key)[0].astype(jnp.bfloat16)


def draw_window_key(key, part):
    return pair_window(key)[1].astype(jnp.bfloat16)


def draw_grid_query(key, part):
    return pair_grid(key)[0].astype(jnp.bfloat16)


def draw_grid_key(key, part):
    return pair_grid(key)[1].astype(jnp.bfloat16)


def draw_query_gain(key, part):
    return grid_gain(key, 303)


def draw_key_gain(key, part):
    return grid_gain(key, 404)


def steps_of(rng, dims, shards, low, high):
    def one(dim, blocks):
        heights = jax.random.uniform(jax.random.fold_in(jax.random.fold_in(rng, 6), dim), (blocks,), jnp.float32, low / len(shards), high / len(shards))
        return jnp.repeat(jnp.exp(heights), dims[dim] // blocks).reshape((-1,) + (1,) * (len(dims) - dim - 1))

    loudness = one(*shards[0])
    for cut in shards[1:]:
        loudness = loudness * one(*cut)
    return loudness


def noise(own_key, extent, scale, most, cuts=(), held_as=jnp.bfloat16):
    entries = scale * jax.random.normal(own_key, extent, jnp.float32)
    if cuts:
        entries = entries * steps_of(own_key, extent, cuts, -0.22, 0.18)
    return jnp.clip(entries, -most, most).astype(held_as)


def setup_inputs(seed: int = 0, part: int = 0) -> dict:
    key_list = jax.random.split(jax.random.key(seed), 12)
    part_keys = jax.random.split(jax.random.fold_in(key_list[11], part), 12)
    return {
        "window_query": draw_window_query(jax.random.fold_in(jax.random.fold_in(key_list[11], part), 71), part),
        "window_key": draw_window_key(jax.random.fold_in(jax.random.fold_in(key_list[11], part), 71), part),
        "window_value": noise(part_keys[2], (TOKENS, KVH_A * HEAD), 1.0, 6.0, ((0, 32), (1, 8))),
        "grid_query": draw_grid_query(jax.random.fold_in(jax.random.fold_in(key_list[11], part), 71), part),
        "grid_key": draw_grid_key(jax.random.fold_in(jax.random.fold_in(key_list[11], part), 71), part),
        "grid_value": noise(part_keys[5], (TOKENS, KVH_B * HEAD), 1.0, 6.0, ((0, 32), (1, 8))),
        "sink_logit": jnp.clip(1.0 + 5.0 * jax.random.uniform(key_list[6], (QH_A,), jnp.float32) ** steps_of(key_list[6], (QH_A,), ((0, 8),), -0.2, 0.2), 1.0, 6.0),
        "query_gain": draw_query_gain(jax.random.fold_in(key_list[11], 71), part),
        "key_gain": draw_key_gain(jax.random.fold_in(key_list[11], 71), part),
        "window_weights": noise(key_list[9], (QH_A * HEAD, D), 0.1, 0.59765625, ((0, 8),)),
        "grid_weights": noise(key_list[10], (QH_B * HEAD, D), 0.1, 0.59765625, ((0, 8),)),
    }


THETA = 10000.0
NEGATIVE = -1e+30
EPSILON = 1e-06

def turn_section(values, places):
    width = values.shape[-1]
    half_width = width // 2
    frequency = THETA ** (-jnp.arange(0, width, 2, dtype=jnp.float32) / width)
    angles = places[:, None] * frequency[None, :]
    cosine = jnp.cos(angles)[:, None, :]
    sine_part = jnp.sin(angles)[:, None, :]
    first_half = values[..., :half_width]
    second_half = values[..., half_width:]
    return jnp.concatenate([first_half * cosine - second_half * sine_part, second_half * cosine + first_half * sine_part], axis=-1)

def normed_turn(values, gain, places):
    count_rows = values.shape[0]
    shaped = values.astype(jnp.float32).reshape(count_rows, -1, HEAD)
    scaled = shaped * lax.rsqrt(lax.optimization_barrier(jnp.mean(shaped * shaped, axis=-1, keepdims=True)) + EPSILON)
    scaled = scaled * gain.astype(jnp.float32)
    grid_row = (places // GRID_W).astype(jnp.float32)
    grid_col = (places % GRID_W).astype(jnp.float32)
    section = HEAD // 2
    turned = jnp.concatenate([turn_section(scaled[..., :section], grid_row), turn_section(scaled[..., section:], grid_col)], axis=-1)
    return turned.astype(jnp.bfloat16)

def window_attend(queries, keys_pad, values_pad, slopes, sink_logits, offset, total_rows):
    query_rows = queries.shape[0]
    block_span = WINDOW // 2
    blocks = query_rows // block_span
    key_heads = keys_pad.shape[1] // HEAD
    group_size = queries.shape[1] // keys_pad.shape[1]
    query_blocks = queries.astype(jnp.float32).reshape(blocks, block_span, key_heads, group_size, HEAD)
    key_blocks = keys_pad.astype(jnp.float32).reshape(blocks + 4, block_span, key_heads, HEAD)
    value_blocks = values_pad.astype(jnp.float32).reshape(blocks + 4, block_span, key_heads, HEAD)
    key_window = jnp.concatenate([key_blocks[block_shift:block_shift + blocks] for block_shift in range(5)], axis=1)
    value_window = jnp.concatenate([value_blocks[block_shift:block_shift + blocks] for block_shift in range(5)], axis=1)
    scores = jnp.einsum('nqkgd,nskd->kgnqs', query_blocks, key_window) * HEAD ** (-0.5)
    query_place = offset + jnp.arange(query_rows, dtype=jnp.int32).reshape(blocks, block_span, 1)
    key_place = offset - WINDOW + block_span * jnp.arange(blocks, dtype=jnp.int32)[:, None, None] + jnp.arange(5 * block_span, dtype=jnp.int32)[None, None, :]
    distance = jnp.abs(key_place - query_place)
    inside = (distance <= WINDOW) & (key_place >= 0) & (key_place < total_rows)
    slope_grid = slopes.reshape(key_heads, group_size, 1, 1, 1)
    sink_grid = sink_logits.astype(jnp.float32).reshape(key_heads, group_size, 1, 1)
    scores = jnp.where(inside, scores - slope_grid * distance.astype(jnp.float32), NEGATIVE)
    highest = jnp.maximum(lax.optimization_barrier(jnp.max(scores, axis=-1)), sink_grid)
    raised = jnp.exp(scores - highest[..., None])
    denominator = lax.optimization_barrier(jnp.sum(raised, axis=-1)) + jnp.exp(sink_grid - highest)
    weights = lax.optimization_barrier((raised / denominator[..., None]).astype(jnp.bfloat16))
    attended = jnp.einsum('kgnqs,nskd->nqkgd', weights.astype(jnp.float32), value_window)
    return attended.astype(jnp.bfloat16).reshape(query_rows, -1)

def reference(window_query, window_key, window_value, grid_query, grid_key, grid_value, sink_logit, query_gain, key_gain, window_weights, grid_weights):
    total_rows = window_query.shape[0]
    places = jnp.arange(total_rows, dtype=jnp.int32)
    slopes = 2.0 ** (-8.0 * jnp.arange(1, QH_A + 1, dtype=jnp.float32) / QH_A)
    padding = ((WINDOW, WINDOW), (0, 0))
    window_out = window_attend(window_query, jnp.pad(window_key, padding), jnp.pad(window_value, padding), slopes, sink_logit, 0, total_rows)
    group_size = QH_B // KVH_B
    turned_q = lax.optimization_barrier(normed_turn(grid_query, query_gain, places))
    turned_q = turned_q.astype(jnp.float32).reshape(total_rows, KVH_B, group_size, HEAD)
    turned_k = lax.optimization_barrier(normed_turn(grid_key, key_gain, places))
    key_pieces = turned_k.astype(jnp.float32).reshape(N_SP, total_rows // N_SP, KVH_B, HEAD)
    value_pieces = grid_value.astype(jnp.float32).reshape(N_SP, total_rows // N_SP, KVH_B, HEAD)

    def absorb(carry, block_pair):
        highest, summed, gathered = carry
        key_block, value_block = block_pair
        scores = jnp.einsum('tkgd,skd->kgts', turned_q, key_block) * HEAD ** (-0.5)
        raised_top = jnp.maximum(highest, lax.optimization_barrier(jnp.max(scores, axis=-1)))
        fading = jnp.exp(highest - raised_top)
        raised = jnp.exp(scores - raised_top[..., None])
        summed = summed * fading + lax.optimization_barrier(jnp.sum(raised, axis=-1))
        rounded = lax.optimization_barrier(raised.astype(jnp.bfloat16)).astype(jnp.float32)
        gathered = gathered * fading[..., None] + jnp.einsum('kgts,skd->kgtd', rounded, value_block)
        return ((raised_top, summed, gathered), None)
    start_carry = (jnp.full((KVH_B, group_size, total_rows), NEGATIVE, jnp.float32), jnp.zeros((KVH_B, group_size, total_rows), jnp.float32), jnp.zeros((KVH_B, group_size, total_rows, HEAD), jnp.float32))
    final_carry, _ = lax.scan(absorb, start_carry, (key_pieces, value_pieces))
    grid_out = (final_carry[2] / final_carry[1][..., None]).astype(jnp.bfloat16)
    width_a = QH_A // N_TP * HEAD
    heads_b = KVH_B // N_TP
    shaped_b = grid_weights.reshape(KVH_B, group_size, HEAD, D)

    def group_term(running, group_index):
        part_a = lax.dynamic_slice_in_dim(window_out, group_index * width_a, width_a, 1)
        rows_a = lax.dynamic_slice_in_dim(window_weights, group_index * width_a, width_a, 0)
        part_b = lax.dynamic_slice_in_dim(grid_out, group_index * heads_b, heads_b, 0)
        rows_b = lax.dynamic_slice_in_dim(shaped_b, group_index * heads_b, heads_b, 0)
        partial_term = jnp.dot(part_a, rows_a, preferred_element_type=jnp.float32)
        partial_term = partial_term + jnp.einsum('kgtd,kgdo->to', part_b.astype(jnp.float32), rows_b.astype(jnp.float32))
        partial_term = lax.optimization_barrier(partial_term.astype(jnp.bfloat16)).astype(jnp.float32)
        return (running + partial_term, None)
    merged, _ = lax.scan(group_term, jnp.zeros((total_rows, D), jnp.float32), jnp.arange(N_TP, dtype=jnp.int32))
    return merged.astype(jnp.bfloat16)
```

```python
import functools
import math

import jax
import jax.numpy as jnp
from jax import lax
from jax.experimental import pallas as pl
from jax.experimental.pallas import tpu as pltpu
from jax.sharding import Mesh
from jax.sharding import PartitionSpec as P

HEAD = 128
QH_A = 16
WINDOW = 128
GRID_W = 64
THETA = 10000.0
NEGATIVE = -1e30
EPSILON = 1e-06
CORES = 2
PLANES = 2


def turn_tables(offset, local_rows):
    half = HEAD // 4
    frequency = THETA ** (-jnp.arange(0, HEAD // 2, 2, dtype=jnp.float32) / (HEAD // 2))
    places = offset + jnp.arange(local_rows, dtype=jnp.int32)
    row = (places // GRID_W).astype(jnp.float32)[:, None] * frequency[None, :]
    col = (places % GRID_W).astype(jnp.float32)[:, None] * frequency[None, :]
    angles = jnp.concatenate([row, row, col, col], axis=-1)
    lane = jnp.arange(HEAD, dtype=jnp.int32) % (2 * half)
    sign = jnp.where(lane < half, -1.0, 1.0).astype(jnp.float32)
    return jnp.cos(angles), jnp.sin(angles) * sign


def turn_kernel(x_ref, gain_ref, cos_ref, sin_ref, *rest):
    o_ref = rest[-1]
    width = x_ref.shape[1]
    lane = lax.broadcasted_iota(jnp.int32, (x_ref.shape[0], HEAD), 1) % (HEAD // 2)
    for k in range(width // HEAD):
        x = x_ref[:, k * HEAD : (k + 1) * HEAD].astype(jnp.float32)
        scaled = x * lax.rsqrt(jnp.mean(x * x, axis=-1, keepdims=True) + EPSILON)
        scaled = scaled * gain_ref[...]
        up = pltpu.roll(scaled, HEAD // 4, axis=1)
        down = pltpu.roll(scaled, HEAD - HEAD // 4, axis=1)
        other = jnp.where(lane < HEAD // 4, down, up)
        turned = scaled * cos_ref[...] + other * sin_ref[...]
        o_ref[:, k * HEAD : (k + 1) * HEAD] = turned.astype(jnp.bfloat16)
    if len(rest) == 2:
        o_ref[:, width:] = rest[0][...]


def turn(x, gain, cos, sin, beside=None):
    rows, width = x.shape
    args = [x, gain.reshape(1, HEAD), cos, sin]
    if beside is not None:
        args.append(beside)
        width = width + beside.shape[1]
    return pl.pallas_call(
        turn_kernel,
        out_shape=jax.ShapeDtypeStruct((rows, width), jnp.bfloat16),
        cost_estimate=pl.CostEstimate(
            flops=rows * width * 16, bytes_accessed=rows * width * 8, transcendentals=rows
        ),
    )(*args)


def attend_kernel(q_ref, kv_ref, o_ref, rows_ref, top_ref, sum_ref, acc_ref, *, chunks):
    step = pl.program_id(0)
    heads = q_ref.shape[1] // HEAD
    count = q_ref.shape[0]
    factor = math.log2(math.e) * HEAD ** (-0.5)

    @pl.when(step == 0)
    def _():
        for h in range(heads):
            rows_ref[h * count : (h + 1) * count, :] = q_ref[:, h * HEAD : (h + 1) * HEAD]
        top_ref[...] = jnp.full_like(top_ref, NEGATIVE)
        sum_ref[...] = jnp.zeros_like(sum_ref)
        acc_ref[...] = jnp.zeros_like(acc_ref)

    keys = kv_ref[:, :HEAD]
    values = kv_ref[:, HEAD:].T

    def score(lo, hi):
        return lax.dot_general(
            keys,
            rows_ref[lo:hi, :],
            (((1,), (1,)), ((), ())),
            preferred_element_type=jnp.float32,
        )

    def absorb(scores, lo, hi):
        before = top_ref[:, lo:hi]
        top = jnp.maximum(before, jnp.max(scores, axis=0, keepdims=True))
        fading = jnp.exp2((before - top) * factor)
        raised = jnp.exp2((scores - top) * factor)
        top_ref[:, lo:hi] = top
        sum_ref[:, lo:hi] = sum_ref[:, lo:hi] * fading + jnp.sum(raised, axis=0, keepdims=True)
        acc_ref[:, lo:hi] = acc_ref[:, lo:hi] * fading + lax.dot_general(
            values,
            raised.astype(jnp.bfloat16),
            (((1,), (0,)), ((), ())),
            preferred_element_type=jnp.float32,
        )

    waiting = None
    for lo, hi in chunks:
        scores = score(lo, hi)
        if waiting is not None:
            absorb(*waiting)
        waiting = (scores, lo, hi)
    absorb(*waiting)

    @pl.when(step == pl.num_programs(0) - 1)
    def _():
        out = (acc_ref[...] / sum_ref[...]).T.astype(jnp.bfloat16)
        for h in range(heads):
            o_ref[:, h * HEAD : (h + 1) * HEAD] = out[h * count : (h + 1) * count, :]


def attend(queries, kv, block=1024, chunk=256):
    count, width = queries.shape
    total = kv.shape[0]
    while total % block:
        block //= 2
    rows = count * (width // HEAD)
    chunks = tuple((lo, min(lo + chunk, rows)) for lo in range(0, rows, chunk))
    return pl.pallas_call(
        functools.partial(attend_kernel, chunks=chunks),
        grid=(total // block,),
        in_specs=[
            pl.BlockSpec((count, width), lambda i: (0, 0)),
            pl.BlockSpec((block, 2 * HEAD), lambda i: (i, 0)),
        ],
        out_specs=pl.BlockSpec((count, width), lambda i: (0, 0)),
        out_shape=jax.ShapeDtypeStruct((count, width), jnp.bfloat16),
        scratch_shapes=[
            pltpu.VMEM((rows, HEAD), jnp.bfloat16),
            pltpu.VMEM((1, rows), jnp.float32),
            pltpu.VMEM((1, rows), jnp.float32),
            pltpu.VMEM((HEAD, rows), jnp.float32),
        ],
        compiler_params=pltpu.CompilerParams(dimension_semantics=("arbitrary",)),
        cost_estimate=pl.CostEstimate(
            flops=4 * rows * total * HEAD,
            bytes_accessed=total * 2 * HEAD * 2,
            transcendentals=rows * total,
        ),
    )(queries, kv)


def extended(cells, axes, width):
    count = math.prod(lax.axis_size(a) for a in axes)
    ends = count - 1
    head = cells[:, :width]
    tail = cells[:, cells.shape[1] - width :]
    return jnp.concatenate(
        [
            lax.ppermute(tail, axes, [(i, i + 1) for i in range(ends)]),
            cells,
            lax.ppermute(head, axes, [(i + 1, i) for i in range(ends)]),
        ],
        axis=1,
    )


def window_attend(queries, keys_pad, values_pad, slopes, sink_logits, offset, total_rows):
    query_rows = queries.shape[0]
    block_span = WINDOW // 2
    blocks = query_rows // block_span
    key_heads = keys_pad.shape[1] // HEAD
    group_size = queries.shape[1] // keys_pad.shape[1]
    query_blocks = queries.reshape(blocks, block_span, key_heads, group_size, HEAD)
    key_blocks = keys_pad.reshape(blocks + 4, block_span, key_heads, HEAD)
    value_blocks = values_pad.reshape(blocks + 4, block_span, key_heads, HEAD)
    key_window = jnp.concatenate([key_blocks[s : s + blocks] for s in range(5)], axis=1)
    value_window = jnp.concatenate([value_blocks[s : s + blocks] for s in range(5)], axis=1)
    scores = jnp.einsum(
        "nqkgd,nskd->kgnqs", query_blocks, key_window, preferred_element_type=jnp.float32
    ) * HEAD ** (-0.5)
    query_place = offset + jnp.arange(query_rows, dtype=jnp.int32).reshape(blocks, block_span, 1)
    key_place = (
        offset
        - WINDOW
        + block_span * jnp.arange(blocks, dtype=jnp.int32)[:, None, None]
        + jnp.arange(5 * block_span, dtype=jnp.int32)[None, None, :]
    )
    distance = jnp.abs(key_place - query_place)
    inside = (distance <= WINDOW) & (key_place >= 0) & (key_place < total_rows)
    slope_grid = slopes.reshape(key_heads, group_size, 1, 1, 1)
    sink_grid = sink_logits.reshape(key_heads, group_size, 1, 1)
    scores = jnp.where(inside, scores - slope_grid * distance.astype(jnp.float32), NEGATIVE)
    highest = jnp.maximum(jnp.max(scores, axis=-1), sink_grid)
    raised = jnp.exp(scores - highest[..., None])
    denominator = jnp.sum(raised, axis=-1) + jnp.exp(sink_grid - highest)
    weights = (raised / denominator[..., None]).astype(jnp.bfloat16)
    attended = jnp.einsum(
        "kgnqs,nskd->nqkgd", weights, value_window, preferred_element_type=jnp.float32
    )
    return attended.astype(jnp.bfloat16).reshape(query_rows, -1)


def by_target(rows):
    across = lax.axis_size("x")
    x = lax.axis_index("x")
    core = lax.axis_index("core")
    count = rows.shape[0] // (across * CORES)
    tiles = rows.reshape(across, CORES, count, rows.shape[1])
    tiles = jnp.where(core == 0, tiles, tiles[:, ::-1])
    tiles = lax.dynamic_slice_in_dim(jnp.concatenate([tiles, tiles], axis=0), x, across, axis=0)
    return jnp.swapaxes(tiles, 0, 1).reshape(rows.shape)


def swapped(value):
    across = lax.axis_size("x")
    index = lambda plane, x, core: (plane * across + x) * CORES + core
    pairs = [
        (index(p, x, c), index(c, x, p))
        for p in range(PLANES)
        for x in range(across)
        for c in range(CORES)
    ]
    return lax.ppermute(value, ("lo", "x", "core"), pairs)


def sent_and_summed(partial):
    half = partial.shape[0] // CORES
    across = lax.axis_size("x")
    theirs = lax.ppermute(partial[half:], "core", [(0, 1), (1, 0)])
    both = partial[:half].astype(jnp.float32) + theirs.astype(jnp.float32)
    tiles = both.astype(jnp.bfloat16).reshape(across, half // across, -1)
    total = tiles[0].astype(jnp.float32)
    for d in range(1, across):
        total = total + lax.ppermute(
            tiles[d], "x", [(i, (i + d) % across) for i in range(across)]
        ).astype(jnp.float32)
    return total


def per_device(
    window_query,
    window_key,
    window_value,
    grid_query,
    grid_key,
    grid_value,
    sink_logit,
    query_gain,
    key_gain,
    window_weights,
    grid_weights,
):
    local_rows = window_query.shape[0]
    planes = ("hi", "lo")
    plane = lax.axis_index("hi") * PLANES + lax.axis_index("lo")
    head_group = lax.axis_index("x") * CORES + lax.axis_index("core")
    offset = plane * local_rows
    total_rows = local_rows * lax.axis_size("hi") * PLANES
    cos, sin = turn_tables(offset, local_rows)
    kv = swapped(turn(grid_key, key_gain, cos, sin, grid_value))
    kv_all = lax.all_gather(kv, ("hi", "core"), axis=0, tiled=True)

    kv, cos, sin, grid_query, window_query = lax.optimization_barrier(
        (kv, cos, sin, grid_query, window_query)
    )
    queries = swapped(by_target(turn(grid_query, query_gain, cos, sin)))

    local_heads = sink_logit.shape[0]
    head_number = head_group * local_heads + 1 + jnp.arange(local_heads, dtype=jnp.int32)
    slopes = 2.0 ** (-8.0 * head_number.astype(jnp.float32) / QH_A)
    padded = extended(jnp.stack([window_key, window_value]), planes, WINDOW)
    window_out = by_target(
        window_attend(window_query, padded[0], padded[1], slopes, sink_logit, offset, total_rows)
    )
    grid_out = swapped(attend(queries, kv_all))
    partial = jnp.dot(window_out, window_weights, preferred_element_type=jnp.float32) + jnp.dot(
        grid_out, grid_weights, preferred_element_type=jnp.float32
    )
    return sent_and_summed(partial.astype(jnp.bfloat16)).astype(jnp.bfloat16)


def solution(mesh):
    shape = mesh.shape
    inner = Mesh(
        mesh.devices.reshape(
            shape["grp"], shape["sp"] // PLANES, PLANES, shape["tp"] // CORES, CORES
        ),
        ("grp", "hi", "lo", "x", "core"),
    )
    rows = ("grp", "hi", "lo")
    heads = ("x", "core")
    return jax.shard_map(
        per_device,
        mesh=inner,
        in_specs=(
            P(rows, heads),
            P(rows, heads),
            P(rows, heads),
            P(rows, heads),
            P(rows, heads),
            P(rows, heads),
            P(heads),
            P(),
            P(),
            P(heads, None),
            P(heads, None),
        ),
        out_specs=P(rows + heads, None),
        check_vma=False,
    )
```

```python
import functools
import math

import jax
import jax.numpy as jnp
from jax import lax
from jax.experimental import pallas as pl
from jax.experimental.pallas import tpu as pltpu
from jax.sharding import Mesh
from jax.sharding import PartitionSpec as P

HEAD = 128
QH_A = 16
WINDOW = 128
GRID_W = 64
THETA = 10000.0
NEGATIVE = -1e30
EPSILON = 1e-06
CORES = 2
PLANES = 4
TAIL = 32


def turn_tables(offset, local_rows):
    half = HEAD // 4
    frequency = THETA ** (-jnp.arange(0, HEAD // 2, 2, dtype=jnp.float32) / (HEAD // 2))
    places = offset + jnp.arange(local_rows, dtype=jnp.int32)
    row = (places // GRID_W).astype(jnp.float32)[:, None] * frequency[None, :]
    col = (places % GRID_W).astype(jnp.float32)[:, None] * frequency[None, :]
    angles = jnp.concatenate([row, row, col, col], axis=-1)
    lane = jnp.arange(HEAD, dtype=jnp.int32) % (2 * half)
    sign = jnp.where(lane < half, -1.0, 1.0).astype(jnp.float32)
    return jnp.cos(angles), jnp.sin(angles) * sign


def turn_kernel(x_ref, gain_ref, cos_ref, sin_ref, *rest):
    o_ref = rest[-1]
    width = x_ref.shape[1]
    lane = lax.broadcasted_iota(jnp.int32, (x_ref.shape[0], HEAD), 1) % (HEAD // 2)
    for k in range(width // HEAD):
        x = x_ref[:, k * HEAD : (k + 1) * HEAD].astype(jnp.float32)
        scaled = x * lax.rsqrt(jnp.mean(x * x, axis=-1, keepdims=True) + EPSILON)
        scaled = scaled * gain_ref[...]
        up = pltpu.roll(scaled, HEAD // 4, axis=1)
        down = pltpu.roll(scaled, HEAD - HEAD // 4, axis=1)
        other = jnp.where(lane < HEAD // 4, down, up)
        turned = scaled * cos_ref[...] + other * sin_ref[...]
        o_ref[:, k * HEAD : (k + 1) * HEAD] = turned.astype(jnp.bfloat16)
    if len(rest) == 2:
        o_ref[:, width:] = rest[0][...]


def turn(x, gain, cos, sin, beside=None):
    rows, width = x.shape
    args = [x, gain.reshape(1, HEAD), cos, sin]
    if beside is not None:
        args.append(beside)
        width = width + beside.shape[1]
    return pl.pallas_call(
        turn_kernel,
        out_shape=jax.ShapeDtypeStruct((rows, width), jnp.bfloat16),
        cost_estimate=pl.CostEstimate(
            flops=rows * width * 16, bytes_accessed=rows * width * 8, transcendentals=rows
        ),
    )(*args)


def attend_kernel(*refs, pieces, first, last, chunk):
    q_ref = refs[0]
    kv_refs = refs[1 : 1 + len(pieces)]
    rest = refs[1 + len(pieces) :]
    rows = q_ref.shape[0]
    factor = math.log2(math.e) * HEAD ** (-0.5)
    key_parts = [r[:, :HEAD] for r, kind in zip(kv_refs, pieces) if "k" in kind]
    value_parts = [r[:, r.shape[1] - HEAD :] for r, kind in zip(kv_refs, pieces) if "v" in kind]
    keys = jnp.concatenate(key_parts, axis=0)
    values = jnp.concatenate(value_parts, axis=0).T
    if first:
        before_refs = None
    else:
        before_refs, rest = rest[:3], rest[3:]

    def score(lo):
        return lax.dot_general(
            keys,
            q_ref[lo : lo + chunk, :],
            (((1,), (1,)), ((), ())),
            preferred_element_type=jnp.float32,
        )

    def absorb(scores, lo):
        span = slice(lo, lo + chunk)
        top = jnp.max(scores, axis=0, keepdims=True)
        if not first:
            before = before_refs[0][:, span]
            top = jnp.maximum(before, top)
            fading = jnp.exp2((before - top) * factor)
        raised = jnp.exp2((scores - top) * factor)
        total = jnp.sum(raised, axis=0, keepdims=True)
        acc = lax.dot_general(
            values,
            raised.astype(jnp.bfloat16),
            (((1,), (0,)), ((), ())),
            preferred_element_type=jnp.float32,
        )
        if not first:
            total = total + before_refs[1][:, span] * fading
            acc = acc + before_refs[2][:, span] * fading
        if not last:
            rest[0][:, span] = top
            rest[1][:, span] = total
            rest[2][:, span] = acc
            return
        weight = top * factor + jnp.log2(total)
        high = weight.astype(jnp.bfloat16)
        left = weight - high.astype(jnp.float32)
        middle = left.astype(jnp.bfloat16)
        low = (left - middle.astype(jnp.float32)).astype(jnp.bfloat16)
        terms = [high, middle, low]
        tail = jnp.concatenate(
            [jnp.broadcast_to(t.astype(jnp.float32), (8, chunk)) for t in terms]
            + [jnp.zeros((8, chunk), jnp.float32)],
            axis=0,
        )
        rest[0][:HEAD, span] = (acc / total).astype(jnp.bfloat16)
        rest[0][HEAD:, span] = tail.astype(jnp.bfloat16)

    waiting = None
    for lo in range(0, rows, chunk):
        scores = score(lo)
        if waiting is not None:
            absorb(*waiting)
        waiting = (scores, lo)
    absorb(*waiting)


def attend(queries, kvs, pieces, carry=None, last=False, chunk=256):
    rows = queries.shape[0]
    while rows % chunk:
        chunk //= 2
    keys = sum(a.shape[0] for a, kind in zip(kvs, pieces) if "k" in kind)
    f32 = jnp.float32
    if last:
        out_shape = jax.ShapeDtypeStruct((HEAD + TAIL, rows), jnp.bfloat16)
    else:
        out_shape = (
            jax.ShapeDtypeStruct((1, rows), f32),
            jax.ShapeDtypeStruct((1, rows), f32),
            jax.ShapeDtypeStruct((HEAD, rows), f32),
        )
    return pl.pallas_call(
        functools.partial(
            attend_kernel, pieces=pieces, first=carry is None, last=last, chunk=chunk
        ),
        out_shape=out_shape,
        cost_estimate=pl.CostEstimate(
            flops=4 * rows * keys * HEAD,
            bytes_accessed=rows * HEAD * 10,
            transcendentals=rows * keys,
        ),
    )(queries, *kvs, *(carry or ()))


def merge_kernel(*refs):
    o_ref = refs[-1]
    heads = o_ref.shape[1] // HEAD
    count = o_ref.shape[0]
    parts = refs[:-1]
    weights = [
        r[HEAD : HEAD + 8, :].astype(jnp.float32)[:1]
        + r[HEAD + 8 : HEAD + 16, :].astype(jnp.float32)[:1]
        + r[HEAD + 16 : HEAD + 24, :].astype(jnp.float32)[:1]
        for r in parts
    ]
    top = functools.reduce(jnp.maximum, weights)
    shares = [jnp.exp2(w - top) for w in weights]
    total = functools.reduce(jnp.add, shares)
    out = functools.reduce(
        jnp.add, [r[:HEAD, :].astype(jnp.float32) * s for r, s in zip(parts, shares)]
    )
    out = (out / total).T.astype(jnp.bfloat16)
    for h in range(heads):
        o_ref[:, h * HEAD : (h + 1) * HEAD] = out[h * count : (h + 1) * count, :]


def grid_attend(kv, queries, heads):
    high = lax.axis_size("hi")
    low = lax.axis_size("lo")
    ring = [(i, (i + 1) % high) for i in range(high)]
    back = [(b, a) for a, b in ring]
    ahead = lax.ppermute(kv, "hi", ring)
    behind = lax.ppermute(kv, "hi", back)
    shared = [queries] + [
        lax.ppermute(queries, "lo", [(i, (i + d) % low) for i in range(low)])
        for d in range(1, low)
    ]
    count = queries.shape[0]
    rows = jnp.concatenate(shared, axis=0)
    carry = attend(rows, (kv,), ("kv",))
    for step in range(1, high // 2):
        if step + 1 < high // 2:
            following = (lax.ppermute(ahead, "hi", ring), lax.ppermute(behind, "hi", back))
        else:
            following = (
                lax.ppermute(ahead[:, :HEAD], "hi", ring),
                lax.ppermute(behind[:, HEAD:], "hi", back),
            )
        carry = attend(rows, (ahead, behind), ("kv", "kv"), carry)
        ahead, behind = following
    packed = attend(rows, (ahead, behind), ("k", "v"), carry, last=True)
    parts = [packed[:, :count]] + [
        lax.ppermute(
            packed[:, d * count : (d + 1) * count],
            "lo",
            [(i, (i - d) % low) for i in range(low)],
        )
        for d in range(1, low)
    ]
    return pl.pallas_call(
        merge_kernel,
        out_shape=jax.ShapeDtypeStruct((count // heads, heads * HEAD), jnp.bfloat16),
        cost_estimate=pl.CostEstimate(
            flops=8 * count * HEAD, bytes_accessed=count * HEAD * 10, transcendentals=count
        ),
    )(*parts)


def extended(cells, axes, width):
    count = math.prod(lax.axis_size(a) for a in axes)
    ends = count - 1
    head = cells[:, :width]
    tail = cells[:, cells.shape[1] - width :]
    return jnp.concatenate(
        [
            lax.ppermute(tail, axes, [(i, i + 1) for i in range(ends)]),
            cells,
            lax.ppermute(head, axes, [(i + 1, i) for i in range(ends)]),
        ],
        axis=1,
    )


def window_attend(queries, keys_pad, values_pad, slopes, sink_logits, offset, total_rows):
    query_rows = queries.shape[0]
    block_span = WINDOW // 2
    blocks = query_rows // block_span
    key_heads = keys_pad.shape[1] // HEAD
    group_size = queries.shape[1] // keys_pad.shape[1]
    query_blocks = queries.reshape(blocks, block_span, key_heads, group_size, HEAD)
    key_blocks = keys_pad.reshape(blocks + 4, block_span, key_heads, HEAD)
    value_blocks = values_pad.reshape(blocks + 4, block_span, key_heads, HEAD)
    key_window = jnp.concatenate([key_blocks[s : s + blocks] for s in range(5)], axis=1)
    value_window = jnp.concatenate([value_blocks[s : s + blocks] for s in range(5)], axis=1)
    scores = jnp.einsum(
        "nqkgd,nskd->kgnqs", query_blocks, key_window, preferred_element_type=jnp.float32
    ) * HEAD ** (-0.5)
    query_place = offset + jnp.arange(query_rows, dtype=jnp.int32).reshape(blocks, block_span, 1)
    key_place = (
        offset
        - WINDOW
        + block_span * jnp.arange(blocks, dtype=jnp.int32)[:, None, None]
        + jnp.arange(5 * block_span, dtype=jnp.int32)[None, None, :]
    )
    distance = jnp.abs(key_place - query_place)
    inside = (distance <= WINDOW) & (key_place >= 0) & (key_place < total_rows)
    slope_grid = slopes.reshape(key_heads, group_size, 1, 1, 1)
    sink_grid = sink_logits.reshape(key_heads, group_size, 1, 1)
    scores = jnp.where(inside, scores - slope_grid * distance.astype(jnp.float32), NEGATIVE)
    highest = jnp.maximum(jnp.max(scores, axis=-1), sink_grid)
    raised = jnp.exp(scores - highest[..., None])
    denominator = jnp.sum(raised, axis=-1) + jnp.exp(sink_grid - highest)
    weights = (raised / denominator[..., None]).astype(jnp.bfloat16)
    attended = jnp.einsum(
        "kgnqs,nskd->nqkgd", weights, value_window, preferred_element_type=jnp.float32
    )
    return attended.astype(jnp.bfloat16).reshape(query_rows, -1)


def by_target(rows):
    across = lax.axis_size("x")
    x = lax.axis_index("x")
    core = lax.axis_index("core")
    count = rows.shape[0] // (across * CORES)
    tiles = rows.reshape(across, CORES, count, rows.shape[1])
    tiles = jnp.where(core == 0, tiles, tiles[:, ::-1])
    tiles = lax.dynamic_slice_in_dim(jnp.concatenate([tiles, tiles], axis=0), x, across, axis=0)
    return jnp.swapaxes(tiles, 0, 1).reshape(rows.shape)


def sent_and_summed(partial):
    half = partial.shape[0] // CORES
    across = lax.axis_size("x")
    theirs = lax.ppermute(partial[half:], "core", [(0, 1), (1, 0)])
    both = partial[:half].astype(jnp.float32) + theirs.astype(jnp.float32)
    tiles = both.astype(jnp.bfloat16).reshape(across, half // across, -1)
    total = tiles[0].astype(jnp.float32)
    for d in range(1, across):
        total = total + lax.ppermute(
            tiles[d], "x", [(i, (i + d) % across) for i in range(across)]
        ).astype(jnp.float32)
    return total


def per_device(
    window_query,
    window_key,
    window_value,
    grid_query,
    grid_key,
    grid_value,
    sink_logit,
    query_gain,
    key_gain,
    window_weights,
    grid_weights,
):
    local_rows = window_query.shape[0]
    planes = ("hi", "lo")
    plane = lax.axis_index("hi") * PLANES + lax.axis_index("lo")
    head_group = lax.axis_index("x") * CORES + lax.axis_index("core")
    offset = plane * local_rows
    total_rows = local_rows * lax.axis_size("hi") * PLANES
    cos, sin = turn_tables(offset, local_rows)
    kv = turn(grid_key, key_gain, cos, sin, grid_value)
    heads = grid_query.shape[1] // HEAD
    turned = by_target(turn(grid_query, query_gain, cos, sin))
    queries = jnp.concatenate(
        [turned[:, h * HEAD : (h + 1) * HEAD] for h in range(heads)], axis=0
    )
    grid_out = grid_attend(kv, queries, heads)

    local_heads = sink_logit.shape[0]
    head_number = head_group * local_heads + 1 + jnp.arange(local_heads, dtype=jnp.int32)
    slopes = 2.0 ** (-8.0 * head_number.astype(jnp.float32) / QH_A)
    padded = extended(jnp.stack([window_key, window_value]), planes, WINDOW)
    window_out = by_target(
        window_attend(window_query, padded[0], padded[1], slopes, sink_logit, offset, total_rows)
    )
    partial = jnp.dot(window_out, window_weights, preferred_element_type=jnp.float32) + jnp.dot(
        grid_out, grid_weights, preferred_element_type=jnp.float32
    )
    return sent_and_summed(partial.astype(jnp.bfloat16)).astype(jnp.bfloat16)


def solution(mesh):
    shape = mesh.shape
    inner = Mesh(
        mesh.devices.reshape(
            shape["grp"], shape["sp"] // PLANES, PLANES, shape["tp"] // CORES, CORES
        ),
        ("grp", "hi", "lo", "x", "core"),
    )
    rows = ("grp", "hi", "lo")
    heads = ("x", "core")
    return jax.shard_map(
        per_device,
        mesh=inner,
        in_specs=(
            P(rows, heads),
            P(rows, heads),
            P(rows, heads),
            P(rows, heads),
            P(rows, heads),
            P(rows, heads),
            P(heads),
            P(),
            P(),
            P(heads, None),
            P(heads, None),
        ),
        out_specs=P(rows + heads, None),
        check_vma=False,
    )
```

```python
import functools
import math

import jax
import jax.numpy as jnp
from jax import lax
from jax.experimental import pallas as pl
from jax.experimental.pallas import tpu as pltpu
from jax.sharding import Mesh
from jax.sharding import PartitionSpec as P

HEAD = 128
QH_A = 16
WINDOW = 128
GRID_W = 64
THETA = 10000.0
NEGATIVE = -1e30
EPSILON = 1e-06
CORES = 2
PLANES = 2
TAIL = 32


def turn_tables(offset, local_rows):
    half = HEAD // 4
    frequency = THETA ** (-jnp.arange(0, HEAD // 2, 2, dtype=jnp.float32) / (HEAD // 2))
    places = offset + jnp.arange(local_rows, dtype=jnp.int32)
    row = (places // GRID_W).astype(jnp.float32)[:, None] * frequency[None, :]
    col = (places % GRID_W).astype(jnp.float32)[:, None] * frequency[None, :]
    angles = jnp.concatenate([row, row, col, col], axis=-1)
    lane = jnp.arange(HEAD, dtype=jnp.int32) % (2 * half)
    sign = jnp.where(lane < half, -1.0, 1.0).astype(jnp.float32)
    return jnp.cos(angles), jnp.sin(angles) * sign


def turn_kernel(x_ref, gain_ref, cos_ref, sin_ref, *rest):
    o_ref = rest[-1]
    width = x_ref.shape[1]
    lane = lax.broadcasted_iota(jnp.int32, (x_ref.shape[0], HEAD), 1) % (HEAD // 2)
    for k in range(width // HEAD):
        x = x_ref[:, k * HEAD : (k + 1) * HEAD].astype(jnp.float32)
        scaled = x * lax.rsqrt(jnp.mean(x * x, axis=-1, keepdims=True) + EPSILON)
        scaled = scaled * gain_ref[...]
        up = pltpu.roll(scaled, HEAD // 4, axis=1)
        down = pltpu.roll(scaled, HEAD - HEAD // 4, axis=1)
        other = jnp.where(lane < HEAD // 4, down, up)
        turned = scaled * cos_ref[...] + other * sin_ref[...]
        o_ref[:, k * HEAD : (k + 1) * HEAD] = turned.astype(jnp.bfloat16)
    if len(rest) == 2:
        o_ref[:, width:] = rest[0][...]


def turn(x, gain, cos, sin, beside=None):
    rows, width = x.shape
    args = [x, gain.reshape(1, HEAD), cos, sin]
    if beside is not None:
        args.append(beside)
        width = width + beside.shape[1]
    return pl.pallas_call(
        turn_kernel,
        out_shape=jax.ShapeDtypeStruct((rows, width), jnp.bfloat16),
        cost_estimate=pl.CostEstimate(
            flops=rows * width * 16, bytes_accessed=rows * width * 8, transcendentals=rows
        ),
    )(*args)


def attend_kernel(q_ref, kv_ref, o_ref, top_ref, sum_ref, acc_ref, *, chunks):
    step = pl.program_id(0)
    rows = q_ref.shape[0]
    factor = math.log2(math.e) * HEAD ** (-0.5)

    @pl.when(step == 0)
    def _():
        top_ref[...] = jnp.full_like(top_ref, NEGATIVE)
        sum_ref[...] = jnp.zeros_like(sum_ref)
        acc_ref[...] = jnp.zeros_like(acc_ref)

    keys = kv_ref[:, :HEAD]
    values = kv_ref[:, HEAD:].T

    def score(lo, hi):
        return lax.dot_general(
            keys,
            q_ref[lo:hi, :],
            (((1,), (1,)), ((), ())),
            preferred_element_type=jnp.float32,
        )

    def absorb(scores, lo, hi):
        before = top_ref[:, lo:hi]
        top = jnp.maximum(before, jnp.max(scores, axis=0, keepdims=True))
        fading = jnp.exp2((before - top) * factor)
        raised = jnp.exp2((scores - top) * factor)
        top_ref[:, lo:hi] = top
        sum_ref[:, lo:hi] = sum_ref[:, lo:hi] * fading + jnp.sum(raised, axis=0, keepdims=True)
        acc_ref[:, lo:hi] = acc_ref[:, lo:hi] * fading + lax.dot_general(
            values,
            raised.astype(jnp.bfloat16),
            (((1,), (0,)), ((), ())),
            preferred_element_type=jnp.float32,
        )

    waiting = None
    for lo, hi in chunks:
        scores = score(lo, hi)
        if waiting is not None:
            absorb(*waiting)
        waiting = (scores, lo, hi)
    absorb(*waiting)

    @pl.when(step == pl.num_programs(0) - 1)
    def _():
        weight = top_ref[...] * factor + jnp.log2(sum_ref[...])
        high = weight.astype(jnp.bfloat16)
        left = weight - high.astype(jnp.float32)
        middle = left.astype(jnp.bfloat16)
        low = (left - middle.astype(jnp.float32)).astype(jnp.bfloat16)
        tail = [jnp.broadcast_to(t.astype(jnp.float32), (8, rows)) for t in (high, middle, low)]
        tail.append(jnp.zeros((8, rows), jnp.float32))
        o_ref[:HEAD, :] = (acc_ref[...] / sum_ref[...]).astype(jnp.bfloat16)
        o_ref[HEAD:, :] = jnp.concatenate(tail, axis=0).astype(jnp.bfloat16)


def attend(queries, kv, block=1024, chunk=256):
    rows = queries.shape[0]
    total = kv.shape[0]
    while total % block:
        block //= 2
    chunks = tuple((lo, min(lo + chunk, rows)) for lo in range(0, rows, chunk))
    return pl.pallas_call(
        functools.partial(attend_kernel, chunks=chunks),
        grid=(total // block,),
        in_specs=[
            pl.BlockSpec((rows, HEAD), lambda i: (0, 0)),
            pl.BlockSpec((block, 2 * HEAD), lambda i: (i, 0)),
        ],
        out_specs=pl.BlockSpec((HEAD + TAIL, rows), lambda i: (0, 0)),
        out_shape=jax.ShapeDtypeStruct((HEAD + TAIL, rows), jnp.bfloat16),
        scratch_shapes=[
            pltpu.VMEM((1, rows), jnp.float32),
            pltpu.VMEM((1, rows), jnp.float32),
            pltpu.VMEM((HEAD, rows), jnp.float32),
        ],
        compiler_params=pltpu.CompilerParams(dimension_semantics=("arbitrary",)),
        cost_estimate=pl.CostEstimate(
            flops=4 * rows * total * HEAD,
            bytes_accessed=total * 2 * HEAD * 2,
            transcendentals=rows * total,
        ),
    )(queries, kv)


def merge_kernel(*refs):
    o_ref = refs[-1]
    heads = o_ref.shape[1] // HEAD
    count = o_ref.shape[0]
    parts = refs[:-1]
    weights = [
        r[HEAD : HEAD + 8, :].astype(jnp.float32)[:1]
        + r[HEAD + 8 : HEAD + 16, :].astype(jnp.float32)[:1]
        + r[HEAD + 16 : HEAD + 24, :].astype(jnp.float32)[:1]
        for r in parts
    ]
    top = functools.reduce(jnp.maximum, weights)
    shares = [jnp.exp2(w - top) for w in weights]
    total = functools.reduce(jnp.add, shares)
    out = functools.reduce(
        jnp.add, [r[:HEAD, :].astype(jnp.float32) * s for r, s in zip(parts, shares)]
    )
    out = (out / total).T.astype(jnp.bfloat16)
    for h in range(heads):
        o_ref[:, h * HEAD : (h + 1) * HEAD] = out[h * count : (h + 1) * count, :]


def merged_parts(parts, heads):
    count = parts[0].shape[1]
    return pl.pallas_call(
        merge_kernel,
        out_shape=jax.ShapeDtypeStruct((count // heads, heads * HEAD), jnp.bfloat16),
        cost_estimate=pl.CostEstimate(
            flops=8 * count * HEAD, bytes_accessed=count * HEAD * 10, transcendentals=count
        ),
    )(*parts)


def extended(cells, axes, width):
    count = math.prod(lax.axis_size(a) for a in axes)
    ends = count - 1
    head = cells[:, :width]
    tail = cells[:, cells.shape[1] - width :]
    return jnp.concatenate(
        [
            lax.ppermute(tail, axes, [(i, i + 1) for i in range(ends)]),
            cells,
            lax.ppermute(head, axes, [(i + 1, i) for i in range(ends)]),
        ],
        axis=1,
    )


def window_attend(queries, keys_pad, values_pad, slopes, sink_logits, offset, total_rows):
    query_rows = queries.shape[0]
    block_span = WINDOW // 2
    blocks = query_rows // block_span
    key_heads = keys_pad.shape[1] // HEAD
    group_size = queries.shape[1] // keys_pad.shape[1]
    query_blocks = queries.reshape(blocks, block_span, key_heads, group_size, HEAD)
    key_blocks = keys_pad.reshape(blocks + 4, block_span, key_heads, HEAD)
    value_blocks = values_pad.reshape(blocks + 4, block_span, key_heads, HEAD)
    key_window = jnp.concatenate([key_blocks[s : s + blocks] for s in range(5)], axis=1)
    value_window = jnp.concatenate([value_blocks[s : s + blocks] for s in range(5)], axis=1)
    scores = jnp.einsum(
        "nqkgd,nskd->kgnqs", query_blocks, key_window, preferred_element_type=jnp.float32
    ) * HEAD ** (-0.5)
    query_place = offset + jnp.arange(query_rows, dtype=jnp.int32).reshape(blocks, block_span, 1)
    key_place = (
        offset
        - WINDOW
        + block_span * jnp.arange(blocks, dtype=jnp.int32)[:, None, None]
        + jnp.arange(5 * block_span, dtype=jnp.int32)[None, None, :]
    )
    distance = jnp.abs(key_place - query_place)
    inside = (distance <= WINDOW) & (key_place >= 0) & (key_place < total_rows)
    slope_grid = slopes.reshape(key_heads, group_size, 1, 1, 1)
    sink_grid = sink_logits.reshape(key_heads, group_size, 1, 1)
    scores = jnp.where(inside, scores - slope_grid * distance.astype(jnp.float32), NEGATIVE)
    highest = jnp.maximum(jnp.max(scores, axis=-1), sink_grid)
    raised = jnp.exp(scores - highest[..., None])
    denominator = jnp.sum(raised, axis=-1) + jnp.exp(sink_grid - highest)
    weights = (raised / denominator[..., None]).astype(jnp.bfloat16)
    attended = jnp.einsum(
        "kgnqs,nskd->nqkgd", weights, value_window, preferred_element_type=jnp.float32
    )
    return attended.astype(jnp.bfloat16).reshape(query_rows, -1)


def by_target(rows):
    across = lax.axis_size("x")
    x = lax.axis_index("x")
    core = lax.axis_index("core")
    count = rows.shape[0] // (across * CORES)
    tiles = rows.reshape(across, CORES, count, rows.shape[1])
    tiles = jnp.where(core == 0, tiles, tiles[:, ::-1])
    tiles = lax.dynamic_slice_in_dim(jnp.concatenate([tiles, tiles], axis=0), x, across, axis=0)
    return jnp.swapaxes(tiles, 0, 1).reshape(rows.shape)


def sent_and_summed(partial):
    half = partial.shape[0] // CORES
    across = lax.axis_size("x")
    theirs = lax.ppermute(partial[half:], "core", [(0, 1), (1, 0)])
    both = partial[:half].astype(jnp.float32) + theirs.astype(jnp.float32)
    tiles = both.astype(jnp.bfloat16).reshape(across, half // across, -1)
    total = tiles[0].astype(jnp.float32)
    for d in range(1, across):
        total = total + lax.ppermute(
            tiles[d], "x", [(i, (i + d) % across) for i in range(across)]
        ).astype(jnp.float32)
    return total


def per_device(
    window_query,
    window_key,
    window_value,
    grid_query,
    grid_key,
    grid_value,
    sink_logit,
    query_gain,
    key_gain,
    window_weights,
    grid_weights,
):
    local_rows = window_query.shape[0]
    planes = ("hi", "lo")
    plane = lax.axis_index("hi") * PLANES + lax.axis_index("lo")
    head_group = lax.axis_index("x") * CORES + lax.axis_index("core")
    offset = plane * local_rows
    total_rows = local_rows * lax.axis_size("hi") * PLANES
    cos, sin = turn_tables(offset, local_rows)
    kv = turn(grid_key, key_gain, cos, sin, grid_value)
    kv_all = lax.all_gather(kv, "hi", axis=0, tiled=True)

    kv, cos, sin, grid_query, window_query = lax.optimization_barrier(
        (kv, cos, sin, grid_query, window_query)
    )
    heads = grid_query.shape[1] // HEAD
    turned = by_target(turn(grid_query, query_gain, cos, sin))
    queries = jnp.concatenate(
        [turned[:, h * HEAD : (h + 1) * HEAD] for h in range(heads)], axis=0
    )
    across = [(i, PLANES - 1 - i) for i in range(PLANES)]
    queries_there = lax.ppermute(queries, "lo", across)

    local_heads = sink_logit.shape[0]
    head_number = head_group * local_heads + 1 + jnp.arange(local_heads, dtype=jnp.int32)
    slopes = 2.0 ** (-8.0 * head_number.astype(jnp.float32) / QH_A)
    padded = extended(jnp.stack([window_key, window_value]), planes, WINDOW)
    window_out = by_target(
        window_attend(window_query, padded[0], padded[1], slopes, sink_logit, offset, total_rows)
    )
    part_there = attend(queries_there, kv_all)
    part_back = lax.ppermute(part_there, "lo", across)
    grid_out = merged_parts((attend(queries, kv_all), part_back), heads)
    partial = jnp.dot(window_out, window_weights, preferred_element_type=jnp.float32) + jnp.dot(
        grid_out, grid_weights, preferred_element_type=jnp.float32
    )
    return sent_and_summed(partial.astype(jnp.bfloat16)).astype(jnp.bfloat16)


def solution(mesh):
    shape = mesh.shape
    inner = Mesh(
        mesh.devices.reshape(
            shape["grp"], shape["sp"] // PLANES, PLANES, shape["tp"] // CORES, CORES
        ),
        ("grp", "hi", "lo", "x", "core"),
    )
    rows = ("grp", "hi", "lo")
    heads = ("x", "core")
    return jax.shard_map(
        per_device,
        mesh=inner,
        in_specs=(
            P(rows, heads),
            P(rows, heads),
            P(rows, heads),
            P(rows, heads),
            P(rows, heads),
            P(rows, heads),
            P(heads),
            P(),
            P(),
            P(heads, None),
            P(heads, None),
        ),
        out_specs=P(rows + heads, None),
        check_vma=False,
    )
```

```python
import functools
import math

import jax
import jax.numpy as jnp
from jax import lax
from jax.experimental import pallas as pl
from jax.experimental.pallas import tpu as pltpu
from jax.sharding import Mesh
from jax.sharding import PartitionSpec as P

HEAD = 128
QH_A = 16
WINDOW = 128
GRID_W = 64
THETA = 10000.0
NEGATIVE = -1e30
EPSILON = 1e-06
CORES = 2
PLANES = 4
TAIL = 32


def turn_tables(offset, local_rows):
    half = HEAD // 4
    frequency = THETA ** (-jnp.arange(0, HEAD // 2, 2, dtype=jnp.float32) / (HEAD // 2))
    places = offset + jnp.arange(local_rows, dtype=jnp.int32)
    row = (places // GRID_W).astype(jnp.float32)[:, None] * frequency[None, :]
    col = (places % GRID_W).astype(jnp.float32)[:, None] * frequency[None, :]
    angles = jnp.concatenate([row, row, col, col], axis=-1)
    lane = jnp.arange(HEAD, dtype=jnp.int32) % (2 * half)
    sign = jnp.where(lane < half, -1.0, 1.0).astype(jnp.float32)
    return jnp.cos(angles), jnp.sin(angles) * sign


def turn_kernel(x_ref, gain_ref, cos_ref, sin_ref, *rest):
    o_ref = rest[-1]
    width = x_ref.shape[1]
    lane = lax.broadcasted_iota(jnp.int32, (x_ref.shape[0], HEAD), 1) % (HEAD // 2)
    for k in range(width // HEAD):
        x = x_ref[:, k * HEAD : (k + 1) * HEAD].astype(jnp.float32)
        scaled = x * lax.rsqrt(jnp.mean(x * x, axis=-1, keepdims=True) + EPSILON)
        scaled = scaled * gain_ref[...]
        up = pltpu.roll(scaled, HEAD // 4, axis=1)
        down = pltpu.roll(scaled, HEAD - HEAD // 4, axis=1)
        other = jnp.where(lane < HEAD // 4, down, up)
        turned = scaled * cos_ref[...] + other * sin_ref[...]
        o_ref[:, k * HEAD : (k + 1) * HEAD] = turned.astype(jnp.bfloat16)
    if len(rest) == 2:
        o_ref[:, width:] = rest[0][...]


def turn(x, gain, cos, sin, beside=None):
    rows, width = x.shape
    args = [x, gain.reshape(1, HEAD), cos, sin]
    if beside is not None:
        args.append(beside)
        width = width + beside.shape[1]
    return pl.pallas_call(
        turn_kernel,
        out_shape=jax.ShapeDtypeStruct((rows, width), jnp.bfloat16),
        cost_estimate=pl.CostEstimate(
            flops=rows * width * 16, bytes_accessed=rows * width * 8, transcendentals=rows
        ),
    )(*args)


def attend_kernel(*refs, planes, pieces, last, chunk):
    first = planes > 1
    q_refs, refs = refs[:planes], refs[planes:]
    kv_refs, rest = refs[: len(pieces)], refs[len(pieces) :]
    factor = math.log2(math.e) * HEAD ** (-0.5)
    key_parts = [r[:, :HEAD] for r, kind in zip(kv_refs, pieces) if "k" in kind]
    value_parts = [r[:, r.shape[1] - HEAD :] for r, kind in zip(kv_refs, pieces) if "v" in kind]
    keys = jnp.concatenate(key_parts, axis=0)
    values = jnp.concatenate(value_parts, axis=0).T
    if first:
        before_refs = None
        q_ref = rest[3]
        count = q_refs[0].shape[0]
        for d in range(planes):
            q_ref[d * count : (d + 1) * count, :] = q_refs[d][...]
    else:
        q_ref = q_refs[0]
        before_refs, rest = rest[:3], rest[3:]
    rows = q_ref.shape[0]

    def score(lo):
        return lax.dot_general(
            keys,
            q_ref[lo : lo + chunk, :],
            (((1,), (1,)), ((), ())),
            preferred_element_type=jnp.float32,
        )

    def absorb(scores, lo):
        span = slice(lo, lo + chunk)
        top = jnp.max(scores, axis=0, keepdims=True)
        if not first:
            before = before_refs[0][:, span]
            top = jnp.maximum(before, top)
            fading = jnp.exp2((before - top) * factor)
        raised = jnp.exp2((scores - top) * factor)
        total = jnp.sum(raised, axis=0, keepdims=True)
        acc = lax.dot_general(
            values,
            raised.astype(jnp.bfloat16),
            (((1,), (0,)), ((), ())),
            preferred_element_type=jnp.float32,
        )
        if not first:
            total = total + before_refs[1][:, span] * fading
            acc = acc + before_refs[2][:, span] * fading
        if not last:
            rest[0][:, span] = top
            rest[1][:, span] = total
            rest[2][:, span] = acc
            return
        weight = top * factor + jnp.log2(total)
        high = weight.astype(jnp.bfloat16)
        left = weight - high.astype(jnp.float32)
        middle = left.astype(jnp.bfloat16)
        low = (left - middle.astype(jnp.float32)).astype(jnp.bfloat16)
        terms = [high, middle, low]
        tail = jnp.concatenate(
            [jnp.broadcast_to(t.astype(jnp.float32), (8, chunk)) for t in terms]
            + [jnp.zeros((8, chunk), jnp.float32)],
            axis=0,
        )
        out = (acc / total).astype(jnp.bfloat16)
        tail = tail.astype(jnp.bfloat16)
        each = rows // len(rest)
        for d in range(len(rest)):
            start, stop = max(lo, d * each), min(lo + chunk, (d + 1) * each)
            if start < stop:
                there = slice(start - d * each, stop - d * each)
                rest[d][:HEAD, there] = out[:, start - lo : stop - lo]
                rest[d][HEAD:, there] = tail[:, start - lo : stop - lo]

    waiting = None
    for lo in range(0, rows, chunk):
        scores = score(lo)
        if waiting is not None:
            absorb(*waiting)
        waiting = (scores, lo)
    absorb(*waiting)


def attend(queries, kvs, pieces, carry=None, parts=0, chunk=256):
    rows = sum(q.shape[0] for q in queries)
    while rows % chunk:
        chunk //= 2
    keys = sum(a.shape[0] for a, kind in zip(kvs, pieces) if "k" in kind)
    f32 = jnp.float32
    if parts:
        part = jax.ShapeDtypeStruct((HEAD + TAIL, rows // parts), jnp.bfloat16)
        out_shape = (part,) * parts
    else:
        out_shape = (
            jax.ShapeDtypeStruct((1, rows), f32),
            jax.ShapeDtypeStruct((1, rows), f32),
            jax.ShapeDtypeStruct((HEAD, rows), f32),
        )
    if carry is None:
        out_shape = out_shape + (jax.ShapeDtypeStruct((rows, HEAD), jnp.bfloat16),)
    return pl.pallas_call(
        functools.partial(
            attend_kernel, planes=len(queries), pieces=pieces, last=parts > 0, chunk=chunk
        ),
        out_shape=out_shape,
        cost_estimate=pl.CostEstimate(
            flops=4 * rows * keys * HEAD,
            bytes_accessed=rows * HEAD * 10,
            transcendentals=rows * keys,
        ),
    )(*queries, *kvs, *(carry or ()))


def merge_kernel(*refs):
    o_ref = refs[-1]
    heads = o_ref.shape[1] // HEAD
    count = o_ref.shape[0]
    parts = refs[:-1]
    weights = [
        r[HEAD : HEAD + 8, :].astype(jnp.float32)[:1]
        + r[HEAD + 8 : HEAD + 16, :].astype(jnp.float32)[:1]
        + r[HEAD + 16 : HEAD + 24, :].astype(jnp.float32)[:1]
        for r in parts
    ]
    top = functools.reduce(jnp.maximum, weights)
    shares = [jnp.exp2(w - top) for w in weights]
    total = functools.reduce(jnp.add, shares)
    out = functools.reduce(
        jnp.add, [r[:HEAD, :].astype(jnp.float32) * s for r, s in zip(parts, shares)]
    )
    out = (out / total).T.astype(jnp.bfloat16)
    for h in range(heads):
        o_ref[:, h * HEAD : (h + 1) * HEAD] = out[h * count : (h + 1) * count, :]


def grid_attend(kv, make_queries, heads, held):
    high = lax.axis_size("hi")
    low = lax.axis_size("lo")
    ring = [(i, (i + 1) % high) for i in range(high)]
    back = [(b, a) for a, b in ring]

    ahead = lax.ppermute(kv, "hi", ring)
    behind = lax.ppermute(kv, "hi", back)
    queries = make_queries(kv)
    shared = [queries] + [
        lax.ppermute(queries, "lo", [(i, (i + d) % low) for i in range(low)])
        for d in range(1, low)
    ]
    ahead, behind, held = lax.optimization_barrier((ahead, behind, held))
    rows, carry, waiting = shared, None, (kv,)
    for step in range(1, high // 2):
        if step + 1 < high // 2:
            next_ahead, next_behind = ahead, behind
        else:
            next_ahead, next_behind = ahead[:, :HEAD], behind[:, HEAD:]
        following = (lax.ppermute(next_ahead, "hi", ring), lax.ppermute(next_behind, "hi", back))
        blocks = waiting + (ahead, behind)
        result = attend(rows, blocks, ("kv",) * len(blocks), carry)
        carry, waiting = result[:3], ()
        if step == 1:
            rows = result[3:]
        ahead, behind = following
    parts = attend(rows, (ahead, behind), ("k", "v"), carry, parts=low)
    parts = [parts[0]] + [
        lax.ppermute(parts[d], "lo", [(i, (i - d) % low) for i in range(low)])
        for d in range(1, low)
    ]
    count = parts[0].shape[1]
    grid_out = pl.pallas_call(
        merge_kernel,
        out_shape=jax.ShapeDtypeStruct((count // heads, heads * HEAD), jnp.bfloat16),
        cost_estimate=pl.CostEstimate(
            flops=8 * count * HEAD, bytes_accessed=count * HEAD * 10, transcendentals=count
        ),
    )(*parts)
    return grid_out, held


def extended(cells, axes, width):
    count = math.prod(lax.axis_size(a) for a in axes)
    ends = count - 1
    head = cells[:, :width]
    tail = cells[:, cells.shape[1] - width :]
    above = lax.ppermute(tail, axes, [(i, i + 1) for i in range(ends)])
    below = lax.ppermute(head, axes, [(i + 1, i) for i in range(ends)])
    return jnp.concatenate([above, cells, below], axis=1)


def window_attend(queries, keys_pad, values_pad, slopes, sink_logits, offset, total_rows):
    query_rows = queries.shape[0]
    block_span = WINDOW // 2
    blocks = query_rows // block_span
    key_heads = keys_pad.shape[1] // HEAD
    group_size = queries.shape[1] // keys_pad.shape[1]
    query_blocks = queries.reshape(blocks, block_span, key_heads, group_size, HEAD)
    key_blocks = keys_pad.reshape(blocks + 4, block_span, key_heads, HEAD)
    value_blocks = values_pad.reshape(blocks + 4, block_span, key_heads, HEAD)
    key_window = jnp.concatenate([key_blocks[s : s + blocks] for s in range(5)], axis=1)
    value_window = jnp.concatenate([value_blocks[s : s + blocks] for s in range(5)], axis=1)
    scores = jnp.einsum(
        "nqkgd,nskd->kgnqs", query_blocks, key_window, preferred_element_type=jnp.float32
    ) * HEAD ** (-0.5)
    query_place = offset + jnp.arange(query_rows, dtype=jnp.int32).reshape(blocks, block_span, 1)
    key_place = (
        offset
        - WINDOW
        + block_span * jnp.arange(blocks, dtype=jnp.int32)[:, None, None]
        + jnp.arange(5 * block_span, dtype=jnp.int32)[None, None, :]
    )
    distance = jnp.abs(key_place - query_place)
    inside = (distance <= WINDOW) & (key_place >= 0) & (key_place < total_rows)
    slope_grid = slopes.reshape(key_heads, group_size, 1, 1, 1)
    sink_grid = sink_logits.reshape(key_heads, group_size, 1, 1)
    scores = jnp.where(inside, scores - slope_grid * distance.astype(jnp.float32), NEGATIVE)
    highest = jnp.maximum(jnp.max(scores, axis=-1), sink_grid)
    raised = jnp.exp(scores - highest[..., None])
    denominator = jnp.sum(raised, axis=-1) + jnp.exp(sink_grid - highest)
    weights = (raised / denominator[..., None]).astype(jnp.bfloat16)
    attended = jnp.einsum(
        "kgnqs,nskd->nqkgd", weights, value_window, preferred_element_type=jnp.float32
    )
    return attended.astype(jnp.bfloat16).reshape(query_rows, -1)


def by_target(rows):
    across = lax.axis_size("x")
    core = lax.axis_index("core")
    count = rows.shape[0] // (across * CORES)
    tiles = rows.reshape(across, CORES, count, rows.shape[1])
    tiles = jnp.where(core == 0, tiles, tiles[:, ::-1])
    return jnp.swapaxes(tiles, 0, 1).reshape(rows.shape)


def sent_and_summed(partial):
    half = partial.shape[0] // CORES
    across = lax.axis_size("x")
    theirs = lax.ppermute(partial[half:], "core", [(0, 1), (1, 0)])
    both = partial[:half].astype(jnp.float32) + theirs.astype(jnp.float32)
    tiles = both.astype(jnp.bfloat16).reshape(across, half // across, -1)
    tiles = lax.all_to_all(tiles, "x", 0, 0, tiled=True)
    return jnp.sum(tiles.astype(jnp.float32), axis=0)


def per_device(
    window_query,
    window_key,
    window_value,
    grid_query,
    grid_key,
    grid_value,
    sink_logit,
    query_gain,
    key_gain,
    window_weights,
    grid_weights,
):
    local_rows = window_query.shape[0]
    planes = ("hi", "lo")
    plane = lax.axis_index("hi") * PLANES + lax.axis_index("lo")
    head_group = lax.axis_index("x") * CORES + lax.axis_index("core")
    offset = plane * local_rows
    total_rows = local_rows * lax.axis_size("hi") * PLANES
    cos, sin = turn_tables(offset, local_rows)
    kv = turn(grid_key, key_gain, cos, sin, grid_value)
    heads = grid_query.shape[1] // HEAD

    def make_queries(after):
        _, given = lax.optimization_barrier((after, grid_query))
        turned = by_target(turn(given, query_gain, cos, sin))
        return jnp.concatenate(
            [turned[:, h * HEAD : (h + 1) * HEAD] for h in range(heads)], axis=0
        )

    grid_out, (window_query, window_key, window_value) = grid_attend(
        kv, make_queries, heads, (window_query, window_key, window_value)
    )

    local_heads = sink_logit.shape[0]
    head_number = head_group * local_heads + 1 + jnp.arange(local_heads, dtype=jnp.int32)
    slopes = 2.0 ** (-8.0 * head_number.astype(jnp.float32) / QH_A)
    padded = extended(jnp.stack([window_key, window_value]), planes, WINDOW)
    window_out = by_target(
        window_attend(window_query, padded[0], padded[1], slopes, sink_logit, offset, total_rows)
    )
    partial = jnp.dot(window_out, window_weights, preferred_element_type=jnp.float32) + jnp.dot(
        grid_out, grid_weights, preferred_element_type=jnp.float32
    )
    return sent_and_summed(partial.astype(jnp.bfloat16)).astype(jnp.bfloat16)


def solution(mesh):
    shape = mesh.shape
    inner = Mesh(
        mesh.devices.reshape(
            shape["grp"], shape["sp"] // PLANES, PLANES, shape["tp"] // CORES, CORES
        ),
        ("grp", "hi", "lo", "x", "core"),
    )
    rows = ("grp", "hi", "lo")
    heads = ("x", "core")

    return jax.shard_map(
        per_device,
        mesh=inner,
        in_specs=(
            P(rows, heads),
            P(rows, heads),
            P(rows, heads),
            P(rows, heads),
            P(rows, heads),
            P(rows, heads),
            P(heads),
            P(),
            P(),
            P(heads, None),
            P(heads, None),
        ),
        out_specs=P(rows + heads, None),
        check_vma=False,
    )
```

```python
import functools
import math

import jax
import jax.numpy as jnp
from jax import lax
from jax.experimental import pallas as pl
from jax.experimental.pallas import tpu as pltpu
from jax.sharding import Mesh
from jax.sharding import PartitionSpec as P

HEAD = 128
QH_A = 16
WINDOW = 128
GRID_W = 64
THETA = 10000.0
NEGATIVE = -1e30
EPSILON = 1e-06
CORES = 2
PLANES = 4
TAIL = 16


def turn_tables(offset, local_rows):
    half = HEAD // 4
    frequency = THETA ** (-jnp.arange(0, HEAD // 2, 2, dtype=jnp.float32) / (HEAD // 2))
    places = offset + jnp.arange(local_rows, dtype=jnp.int32)
    row = (places // GRID_W).astype(jnp.float32)[:, None] * frequency[None, :]
    col = (places % GRID_W).astype(jnp.float32)[:, None] * frequency[None, :]
    angles = jnp.concatenate([row, row, col, col], axis=-1)
    lane = jnp.arange(HEAD, dtype=jnp.int32) % (2 * half)
    sign = jnp.where(lane < half, -1.0, 1.0).astype(jnp.float32)
    return jnp.cos(angles), jnp.sin(angles) * sign


def turn_kernel(x_ref, gain_ref, cos_ref, sin_ref, *rest):
    o_ref = rest[-1]
    width = x_ref.shape[1]
    lane = lax.broadcasted_iota(jnp.int32, (x_ref.shape[0], HEAD), 1) % (HEAD // 2)
    for k in range(width // HEAD):
        x = x_ref[:, k * HEAD : (k + 1) * HEAD].astype(jnp.float32)
        scaled = x * lax.rsqrt(jnp.mean(x * x, axis=-1, keepdims=True) + EPSILON)
        scaled = scaled * gain_ref[...]
        up = pltpu.roll(scaled, HEAD // 4, axis=1)
        down = pltpu.roll(scaled, HEAD - HEAD // 4, axis=1)
        other = jnp.where(lane < HEAD // 4, down, up)
        turned = scaled * cos_ref[...] + other * sin_ref[...]
        o_ref[:, k * HEAD : (k + 1) * HEAD] = turned.astype(jnp.bfloat16)
    if len(rest) == 2:
        o_ref[:, width:] = rest[0][...]


def turn(x, gain, cos, sin, beside=None):
    rows, width = x.shape
    args = [x, gain.reshape(1, HEAD), cos, sin]
    if beside is not None:
        args.append(beside)
        width = width + beside.shape[1]
    return pl.pallas_call(
        turn_kernel,
        out_shape=jax.ShapeDtypeStruct((rows, width), jnp.bfloat16),
        cost_estimate=pl.CostEstimate(
            flops=rows * width * 16, bytes_accessed=rows * width * 8, transcendentals=rows
        ),
    )(*args)


def attend_kernel(*refs, planes, pieces, last, chunk):
    first = planes > 1
    q_refs, refs = refs[:planes], refs[planes:]
    kv_refs, rest = refs[: len(pieces)], refs[len(pieces) :]
    factor = math.log2(math.e) * HEAD ** (-0.5)
    key_parts = [r[:, :HEAD] for r, kind in zip(kv_refs, pieces) if "k" in kind]
    value_parts = [r[:, r.shape[1] - HEAD :] for r, kind in zip(kv_refs, pieces) if "v" in kind]
    keys = jnp.concatenate(key_parts, axis=0)
    values = jnp.concatenate(value_parts, axis=0).T
    if first:
        before_refs = None
        q_ref = rest[3]
        count = q_refs[0].shape[0]
        for d in range(planes):
            q_ref[d * count : (d + 1) * count, :] = q_refs[d][...]
    else:
        q_ref = q_refs[0]
        before_refs, rest = rest[:3], rest[3:]
    rows = q_ref.shape[0]

    def score(lo):
        return lax.dot_general(
            keys,
            q_ref[lo : lo + chunk, :],
            (((1,), (1,)), ((), ())),
            preferred_element_type=jnp.float32,
        )

    def absorb(scores, lo):
        span = slice(lo, lo + chunk)
        top = jnp.max(scores, axis=0, keepdims=True)
        if not first:
            before = before_refs[0][:, span]
            top = jnp.maximum(before, top)
            fading = jnp.exp2((before - top) * factor)
        raised = jnp.exp2((scores - top) * factor)
        total = jnp.sum(raised, axis=0, keepdims=True)
        acc = lax.dot_general(
            values,
            raised.astype(jnp.bfloat16),
            (((1,), (0,)), ((), ())),
            preferred_element_type=jnp.float32,
        )
        if not first:
            total = total + before_refs[1][:, span] * fading
            acc = acc + before_refs[2][:, span] * fading
        if not last:
            rest[0][:, span] = top
            rest[1][:, span] = total
            rest[2][:, span] = acc
            return
        weight = top * factor + jnp.log2(total)
        high = weight.astype(jnp.bfloat16)
        left = weight - high.astype(jnp.float32)
        middle = left.astype(jnp.bfloat16)
        low = (left - middle.astype(jnp.float32)).astype(jnp.bfloat16)
        line = lax.broadcasted_iota(jnp.int32, (TAIL, chunk), 0)
        tail = jnp.zeros((TAIL, chunk), jnp.float32)
        for row, term in enumerate((high, middle, low)):
            tail = jnp.where(line == row, term.astype(jnp.float32), tail)
        out = (acc / total).astype(jnp.bfloat16)
        tail = tail.astype(jnp.bfloat16)
        each = rows // len(rest)
        for d in range(len(rest)):
            start, stop = max(lo, d * each), min(lo + chunk, (d + 1) * each)
            if start < stop:
                there = slice(start - d * each, stop - d * each)
                rest[d][:HEAD, there] = out[:, start - lo : stop - lo]
                rest[d][HEAD:, there] = tail[:, start - lo : stop - lo]

    waiting = None
    for lo in range(0, rows, chunk):
        scores = score(lo)
        if waiting is not None:
            absorb(*waiting)
        waiting = (scores, lo)
    absorb(*waiting)


def attend(queries, kvs, pieces, carry=None, parts=0, chunk=256):
    rows = sum(q.shape[0] for q in queries)
    while rows % chunk:
        chunk //= 2
    keys = sum(a.shape[0] for a, kind in zip(kvs, pieces) if "k" in kind)
    f32 = jnp.float32
    if parts:
        part = jax.ShapeDtypeStruct((HEAD + TAIL, rows // parts), jnp.bfloat16)
        out_shape = (part,) * parts
    else:
        out_shape = (
            jax.ShapeDtypeStruct((1, rows), f32),
            jax.ShapeDtypeStruct((1, rows), f32),
            jax.ShapeDtypeStruct((HEAD, rows), f32),
        )
    if carry is None:
        out_shape = out_shape + (jax.ShapeDtypeStruct((rows, HEAD), jnp.bfloat16),)
    return pl.pallas_call(
        functools.partial(
            attend_kernel, planes=len(queries), pieces=pieces, last=parts > 0, chunk=chunk
        ),
        out_shape=out_shape,
        cost_estimate=pl.CostEstimate(
            flops=4 * rows * keys * HEAD,
            bytes_accessed=rows * HEAD * 10,
            transcendentals=rows * keys,
        ),
    )(*queries, *kvs, *(carry or ()))


def project_kernel(*refs, count):
    parts = refs[:count]
    window_ref, window_weights_ref, grid_weights_ref, here_ref, there_ref, grid_ref = refs[count:]

    @pl.when(pl.program_id(0) == 0)
    def _():
        rows = grid_ref.shape[0]
        weights = [
            jnp.sum(r[HEAD:, :].astype(jnp.float32), axis=0, keepdims=True) for r in parts
        ]
        top = functools.reduce(jnp.maximum, weights)
        shares = [jnp.exp2(w - top) for w in weights]
        total = functools.reduce(jnp.add, shares)
        out = functools.reduce(
            jnp.add, [r[:HEAD, :].astype(jnp.float32) * s for r, s in zip(parts, shares)]
        )
        out = (out / total).T.astype(jnp.bfloat16)
        for h in range(grid_ref.shape[1] // HEAD):
            grid_ref[:, h * HEAD : (h + 1) * HEAD] = out[h * rows : (h + 1) * rows, :]

    partial = jnp.dot(
        window_ref[...], window_weights_ref[...], preferred_element_type=jnp.float32
    ) + jnp.dot(grid_ref[...], grid_weights_ref[...], preferred_element_type=jnp.float32)
    half = here_ref.shape[0]
    here_ref[...] = partial[:half].astype(jnp.bfloat16)
    there_ref[...] = partial[half:].astype(jnp.bfloat16)


def project(parts, window_out, window_weights, grid_weights, columns=1024):
    rows, width = window_out.shape
    total = window_weights.shape[1]
    grid_width = grid_weights.shape[0]
    half = jax.ShapeDtypeStruct((rows // CORES, total), jnp.bfloat16)
    whole = lambda a: pl.BlockSpec(a.shape, lambda j: (0, 0))
    return pl.pallas_call(
        functools.partial(project_kernel, count=len(parts)),
        grid=(total // columns,),
        in_specs=[whole(p) for p in parts]
        + [
            whole(window_out),
            pl.BlockSpec((width, columns), lambda j: (0, j)),
            pl.BlockSpec((grid_width, columns), lambda j: (0, j)),
        ],
        out_specs=[pl.BlockSpec((rows // CORES, columns), lambda j: (0, j))] * CORES,
        out_shape=(half,) * CORES,
        scratch_shapes=[pltpu.VMEM((rows, grid_width), jnp.bfloat16)],
        compiler_params=pltpu.CompilerParams(dimension_semantics=("arbitrary",)),
        cost_estimate=pl.CostEstimate(
            flops=2 * rows * (width + grid_width) * total,
            bytes_accessed=2 * total * (width + grid_width + rows),
            transcendentals=rows,
        ),
    )(*parts, window_out, window_weights, grid_weights)


def grid_attend(kv, make_queries, held):
    high = lax.axis_size("hi")
    low = lax.axis_size("lo")
    ring = [(i, (i + 1) % high) for i in range(high)]
    back = [(b, a) for a, b in ring]

    ahead = lax.ppermute(kv, "hi", ring)
    behind = lax.ppermute(kv, "hi", back)
    queries = make_queries(kv)
    shared = [queries] + [
        lax.ppermute(queries, "lo", [(i, (i + d) % low) for i in range(low)])
        for d in range(1, low)
    ]
    ahead, behind, held, shared[0] = lax.optimization_barrier((ahead, behind, held, shared[0]))
    rows, carry, waiting = shared, None, (kv,)
    for step in range(1, high // 2):
        if step + 1 < high // 2:
            next_ahead, next_behind = ahead, behind
        else:
            next_ahead, next_behind = ahead[:, :HEAD], behind[:, HEAD:]
        following = (lax.ppermute(next_ahead, "hi", ring), lax.ppermute(next_behind, "hi", back))
        blocks = waiting + (ahead, behind)
        result = attend(rows, blocks, ("kv",) * len(blocks), carry)
        carry, waiting = result[:3], ()
        if step == 1:
            rows = result[3:]
        ahead, behind = following
    parts = attend(rows, (ahead, behind), ("k", "v"), carry, parts=low)
    parts = [parts[0]] + [
        lax.ppermute(parts[d], "lo", [(i, (i - d) % low) for i in range(low)])
        for d in range(1, low)
    ]
    return parts, held


def extended(cells, axes, width):
    count = math.prod(lax.axis_size(a) for a in axes)
    ends = count - 1
    head = cells[:, :width]
    tail = cells[:, cells.shape[1] - width :]
    above = lax.ppermute(tail, axes, [(i, i + 1) for i in range(ends)])
    below = lax.ppermute(head, axes, [(i + 1, i) for i in range(ends)])
    return jnp.concatenate([above, cells, below], axis=1)


def window_attend(queries, keys_pad, values_pad, slopes, sink_logits, offset, total_rows):
    query_rows = queries.shape[0]
    block_span = WINDOW // 2
    blocks = query_rows // block_span
    key_heads = keys_pad.shape[1] // HEAD
    group_size = queries.shape[1] // keys_pad.shape[1]
    query_blocks = queries.reshape(blocks, block_span, key_heads, group_size, HEAD)
    key_blocks = keys_pad.reshape(blocks + 4, block_span, key_heads, HEAD)
    value_blocks = values_pad.reshape(blocks + 4, block_span, key_heads, HEAD)
    key_window = jnp.concatenate([key_blocks[s : s + blocks] for s in range(5)], axis=1)
    value_window = jnp.concatenate([value_blocks[s : s + blocks] for s in range(5)], axis=1)
    scores = jnp.einsum(
        "nqkgd,nskd->kgnqs", query_blocks, key_window, preferred_element_type=jnp.float32
    ) * HEAD ** (-0.5)
    query_place = offset + jnp.arange(query_rows, dtype=jnp.int32).reshape(blocks, block_span, 1)
    key_place = (
        offset
        - WINDOW
        + block_span * jnp.arange(blocks, dtype=jnp.int32)[:, None, None]
        + jnp.arange(5 * block_span, dtype=jnp.int32)[None, None, :]
    )
    distance = jnp.abs(key_place - query_place)
    inside = (distance <= WINDOW) & (key_place >= 0) & (key_place < total_rows)
    slope_grid = slopes.reshape(key_heads, group_size, 1, 1, 1)
    sink_grid = sink_logits.reshape(key_heads, group_size, 1, 1)
    scores = jnp.where(inside, scores - slope_grid * distance.astype(jnp.float32), NEGATIVE)
    highest = jnp.maximum(jnp.max(scores, axis=-1), sink_grid)
    raised = jnp.exp(scores - highest[..., None])
    denominator = jnp.sum(raised, axis=-1) + jnp.exp(sink_grid - highest)
    weights = (raised / denominator[..., None]).astype(jnp.bfloat16)
    attended = jnp.einsum(
        "kgnqs,nskd->nqkgd", weights, value_window, preferred_element_type=jnp.float32
    )
    return attended.astype(jnp.bfloat16).reshape(query_rows, -1)


def by_target(rows):
    across = lax.axis_size("x")
    x = lax.axis_index("x")
    core = lax.axis_index("core")
    count = rows.shape[0] // (across * CORES)
    tiles = rows.reshape(across, CORES, count, rows.shape[1])
    tiles = jnp.where(core == 0, tiles, tiles[:, ::-1])
    tiles = lax.dynamic_slice_in_dim(jnp.concatenate([tiles, tiles], axis=0), x, across, axis=0)
    return jnp.swapaxes(tiles, 0, 1).reshape(rows.shape)


def sent_and_summed(here, there):
    across = lax.axis_size("x")
    theirs = lax.ppermute(there, "core", [(0, 1), (1, 0)])
    both = here.astype(jnp.float32) + theirs.astype(jnp.float32)
    tiles = both.astype(jnp.bfloat16).reshape(across, here.shape[0] // across, -1)
    total = tiles[0].astype(jnp.float32)
    for d in range(1, across):
        total = total + lax.ppermute(
            tiles[d], "x", [(i, (i + d) % across) for i in range(across)]
        ).astype(jnp.float32)
    return total


def per_device(
    window_query,
    window_key,
    window_value,
    grid_query,
    grid_key,
    grid_value,
    sink_logit,
    query_gain,
    key_gain,
    window_weights,
    grid_weights,
):
    local_rows = window_query.shape[0]
    planes = ("hi", "lo")
    plane = lax.axis_index("hi") * PLANES + lax.axis_index("lo")
    head_group = lax.axis_index("x") * CORES + lax.axis_index("core")
    offset = plane * local_rows
    total_rows = local_rows * lax.axis_size("hi") * PLANES
    cos, sin = turn_tables(offset, local_rows)
    kv = turn(grid_key, key_gain, cos, sin, grid_value)
    heads = grid_query.shape[1] // HEAD

    def make_queries(after):
        _, given = lax.optimization_barrier((after, grid_query))
        turned = by_target(turn(given, query_gain, cos, sin))
        return jnp.concatenate(
            [turned[:, h * HEAD : (h + 1) * HEAD] for h in range(heads)], axis=0
        )

    parts, (window_query, window_key, window_value) = grid_attend(
        kv, make_queries, (window_query, window_key, window_value)
    )

    local_heads = sink_logit.shape[0]
    head_number = head_group * local_heads + 1 + jnp.arange(local_heads, dtype=jnp.int32)
    slopes = 2.0 ** (-8.0 * head_number.astype(jnp.float32) / QH_A)
    padded = extended(jnp.stack([window_key, window_value]), planes, WINDOW)
    window_out = by_target(
        window_attend(window_query, padded[0], padded[1], slopes, sink_logit, offset, total_rows)
    )
    here, there = project(parts, window_out, window_weights, grid_weights)
    return sent_and_summed(here, there).astype(jnp.bfloat16)


def solution(mesh):
    shape = mesh.shape
    inner = Mesh(
        mesh.devices.reshape(
            shape["grp"], shape["sp"] // PLANES, PLANES, shape["tp"] // CORES, CORES
        ),
        ("grp", "hi", "lo", "x", "core"),
    )
    rows = ("grp", "hi", "lo")
    heads = ("x", "core")

    return jax.shard_map(
        per_device,
        mesh=inner,
        in_specs=(
            P(rows, heads),
            P(rows, heads),
            P(rows, heads),
            P(rows, heads),
            P(rows, heads),
            P(rows, heads),
            P(heads),
            P(),
            P(),
            P(heads, None),
            P(heads, None),
        ),
        out_specs=P(rows + heads, None),
        check_vma=False,
    )
```

```python
import functools
import math

import jax
import jax.numpy as jnp
from jax import lax
from jax.experimental import pallas as pl
from jax.experimental.pallas import tpu as pltpu
from jax.sharding import Mesh
from jax.sharding import PartitionSpec as P

HEAD = 128
QH_A = 16
WINDOW = 128
GRID_W = 64
THETA = 10000.0
NEGATIVE = -1e30
EPSILON = 1e-06
CORES = 2
PLANES = 4
TAIL = 16
TURN_VMEM = 8 << 20
ATTEND_VMEM = 24 << 20
PROJECT_VMEM = 24 << 20


def turn_tables(offset, local_rows):
    half = HEAD // 4
    frequency = THETA ** (-jnp.arange(0, HEAD // 2, 2, dtype=jnp.float32) / (HEAD // 2))
    places = offset + jnp.arange(local_rows, dtype=jnp.int32)
    row = (places // GRID_W).astype(jnp.float32)[:, None] * frequency[None, :]
    col = (places % GRID_W).astype(jnp.float32)[:, None] * frequency[None, :]
    angles = jnp.concatenate([row, row, col, col], axis=-1)
    lane = jnp.arange(HEAD, dtype=jnp.int32) % (2 * half)
    sign = jnp.where(lane < half, -1.0, 1.0).astype(jnp.float32)
    return jnp.cos(angles), jnp.sin(angles) * sign


def turn_kernel(x_ref, gain_ref, cos_ref, sin_ref, *rest):
    o_ref = rest[-1]
    width = x_ref.shape[1]
    lane = lax.broadcasted_iota(jnp.int32, (x_ref.shape[0], HEAD), 1) % (HEAD // 2)
    for k in range(width // HEAD):
        x = x_ref[:, k * HEAD : (k + 1) * HEAD].astype(jnp.float32)
        scaled = x * lax.rsqrt(jnp.mean(x * x, axis=-1, keepdims=True) + EPSILON)
        scaled = scaled * gain_ref[...]
        up = pltpu.roll(scaled, HEAD // 4, axis=1)
        down = pltpu.roll(scaled, HEAD - HEAD // 4, axis=1)
        other = jnp.where(lane < HEAD // 4, down, up)
        turned = scaled * cos_ref[...] + other * sin_ref[...]
        o_ref[:, k * HEAD : (k + 1) * HEAD] = turned.astype(jnp.bfloat16)
    if len(rest) == 2:
        o_ref[:, width:] = rest[0][...]


def turn(x, gain, cos, sin, beside=None):
    rows, width = x.shape
    args = [x, gain.reshape(1, HEAD), cos, sin]
    if beside is not None:
        args.append(beside)
        width = width + beside.shape[1]
    return pl.pallas_call(
        turn_kernel,
        out_shape=jax.ShapeDtypeStruct((rows, width), jnp.bfloat16),
        compiler_params=pltpu.CompilerParams(vmem_limit_bytes=TURN_VMEM),
        cost_estimate=pl.CostEstimate(
            flops=rows * width * 16, bytes_accessed=rows * width * 8, transcendentals=rows
        ),
    )(*args)


def attend_kernel(*refs, planes, pieces, last, chunk):
    first = planes > 1
    q_refs, refs = refs[:planes], refs[planes:]
    kv_refs, rest = refs[: len(pieces)], refs[len(pieces) :]
    factor = math.log2(math.e) * HEAD ** (-0.5)
    key_parts = [r[:, :HEAD] for r, kind in zip(kv_refs, pieces) if "k" in kind]
    value_parts = [r[:, r.shape[1] - HEAD :] for r, kind in zip(kv_refs, pieces) if "v" in kind]
    keys = jnp.concatenate(key_parts, axis=0)
    values = jnp.concatenate(value_parts, axis=0).T
    if first:
        before_refs = None
        q_ref = rest[3]
        count = q_refs[0].shape[0]
        for d in range(planes):
            q_ref[d * count : (d + 1) * count, :] = q_refs[d][...]
    else:
        q_ref = q_refs[0]
        before_refs, rest = rest[:3], rest[3:]
    rows = q_ref.shape[0]

    def score(lo):
        return lax.dot_general(
            keys,
            q_ref[lo : lo + chunk, :],
            (((1,), (1,)), ((), ())),
            preferred_element_type=jnp.float32,
        )

    def absorb(scores, lo):
        span = slice(lo, lo + chunk)
        top = jnp.max(scores, axis=0, keepdims=True)
        if not first:
            before = before_refs[0][:, span]
            top = jnp.maximum(before, top)
            fading = jnp.exp2((before - top) * factor)
        raised = jnp.exp2((scores - top) * factor)
        total = jnp.sum(raised, axis=0, keepdims=True)
        acc = lax.dot_general(
            values,
            raised.astype(jnp.bfloat16),
            (((1,), (0,)), ((), ())),
            preferred_element_type=jnp.float32,
        )
        if not first:
            total = total + before_refs[1][:, span] * fading
            acc = acc + before_refs[2][:, span] * fading
        if not last:
            rest[0][:, span] = top
            rest[1][:, span] = total
            rest[2][:, span] = acc
            return
        weight = top * factor + jnp.log2(total)
        high = weight.astype(jnp.bfloat16)
        left = weight - high.astype(jnp.float32)
        middle = left.astype(jnp.bfloat16)
        low = (left - middle.astype(jnp.float32)).astype(jnp.bfloat16)
        line = lax.broadcasted_iota(jnp.int32, (TAIL, chunk), 0)
        tail = jnp.zeros((TAIL, chunk), jnp.float32)
        for row, term in enumerate((high, middle, low)):
            tail = jnp.where(line == row, term.astype(jnp.float32), tail)
        out = (acc / total).astype(jnp.bfloat16)
        tail = tail.astype(jnp.bfloat16)
        each = rows // len(rest)
        for d in range(len(rest)):
            start, stop = max(lo, d * each), min(lo + chunk, (d + 1) * each)
            if start < stop:
                there = slice(start - d * each, stop - d * each)
                rest[d][:HEAD, there] = out[:, start - lo : stop - lo]
                rest[d][HEAD:, there] = tail[:, start - lo : stop - lo]

    waiting = None
    for lo in range(0, rows, chunk):
        scores = score(lo)
        if waiting is not None:
            absorb(*waiting)
        waiting = (scores, lo)
    absorb(*waiting)


def attend(queries, kvs, pieces, carry=None, parts=0, chunk=256):
    rows = sum(q.shape[0] for q in queries)
    while rows % chunk:
        chunk //= 2
    keys = sum(a.shape[0] for a, kind in zip(kvs, pieces) if "k" in kind)
    f32 = jnp.float32
    if parts:
        part = jax.ShapeDtypeStruct((HEAD + TAIL, rows // parts), jnp.bfloat16)
        out_shape = (part,) * parts
    else:
        out_shape = (
            jax.ShapeDtypeStruct((1, rows), f32),
            jax.ShapeDtypeStruct((1, rows), f32),
            jax.ShapeDtypeStruct((HEAD, rows), f32),
        )
    if carry is None:
        out_shape = out_shape + (jax.ShapeDtypeStruct((rows, HEAD), jnp.bfloat16),)
    return pl.pallas_call(
        functools.partial(
            attend_kernel, planes=len(queries), pieces=pieces, last=parts > 0, chunk=chunk
        ),
        out_shape=out_shape,
        compiler_params=pltpu.CompilerParams(vmem_limit_bytes=ATTEND_VMEM),
        cost_estimate=pl.CostEstimate(
            flops=4 * rows * keys * HEAD,
            bytes_accessed=rows * HEAD * 10,
            transcendentals=rows * keys,
        ),
    )(*queries, *kvs, *(carry or ()))


def project_kernel(*refs, count):
    parts = refs[:count]
    window_ref, window_weights_ref, grid_weights_ref, here_ref, there_ref, grid_ref = refs[count:]

    @pl.when(pl.program_id(0) == 0)
    def _():
        rows = grid_ref.shape[0]
        weights = [
            jnp.sum(r[HEAD:, :].astype(jnp.float32), axis=0, keepdims=True) for r in parts
        ]
        top = functools.reduce(jnp.maximum, weights)
        shares = [jnp.exp2(w - top) for w in weights]
        total = functools.reduce(jnp.add, shares)
        out = functools.reduce(
            jnp.add, [r[:HEAD, :].astype(jnp.float32) * s for r, s in zip(parts, shares)]
        )
        out = (out / total).T.astype(jnp.bfloat16)
        for h in range(grid_ref.shape[1] // HEAD):
            grid_ref[:, h * HEAD : (h + 1) * HEAD] = out[h * rows : (h + 1) * rows, :]

    partial = jnp.dot(
        window_ref[...], window_weights_ref[...], preferred_element_type=jnp.float32
    ) + jnp.dot(grid_ref[...], grid_weights_ref[...], preferred_element_type=jnp.float32)
    half = here_ref.shape[0]
    here_ref[...] = partial[:half].astype(jnp.bfloat16)
    there_ref[...] = partial[half:].astype(jnp.bfloat16)


def project(parts, window_out, window_weights, grid_weights, columns=1024):
    rows, width = window_out.shape
    total = window_weights.shape[1]
    grid_width = grid_weights.shape[0]
    half = jax.ShapeDtypeStruct((rows // CORES, total), jnp.bfloat16)
    whole = lambda a: pl.BlockSpec(a.shape, lambda j: (0, 0))
    return pl.pallas_call(
        functools.partial(project_kernel, count=len(parts)),
        grid=(total // columns,),
        in_specs=[whole(p) for p in parts]
        + [
            whole(window_out),
            pl.BlockSpec((width, columns), lambda j: (0, j)),
            pl.BlockSpec((grid_width, columns), lambda j: (0, j)),
        ],
        out_specs=[pl.BlockSpec((rows // CORES, columns), lambda j: (0, j))] * CORES,
        out_shape=(half,) * CORES,
        scratch_shapes=[pltpu.VMEM((rows, grid_width), jnp.bfloat16)],
        compiler_params=pltpu.CompilerParams(
            dimension_semantics=("arbitrary",), vmem_limit_bytes=PROJECT_VMEM
        ),
        cost_estimate=pl.CostEstimate(
            flops=2 * rows * (width + grid_width) * total,
            bytes_accessed=2 * total * (width + grid_width + rows),
            transcendentals=rows,
        ),
    )(*parts, window_out, window_weights, grid_weights)


def grid_attend(kv, make_queries, held):
    high = lax.axis_size("hi")
    low = lax.axis_size("lo")
    ring = [(i, (i + 1) % high) for i in range(high)]
    back = [(b, a) for a, b in ring]

    ahead = lax.ppermute(kv, "hi", ring)
    behind = lax.ppermute(kv, "hi", back)
    queries = make_queries(kv)
    shared = [queries] + [
        lax.ppermute(queries, "lo", [(i, (i + d) % low) for i in range(low)])
        for d in range(1, low)
    ]
    ahead, behind, held, shared[0] = lax.optimization_barrier((ahead, behind, held, shared[0]))
    rows, carry, waiting = shared, None, (kv,)
    for step in range(1, high // 2):
        if step + 1 < high // 2:
            next_ahead, next_behind = ahead, behind
        else:
            next_ahead, next_behind = ahead[:, :HEAD], behind[:, HEAD:]
        following = (lax.ppermute(next_ahead, "hi", ring), lax.ppermute(next_behind, "hi", back))
        blocks = waiting + (ahead, behind)
        result = attend(rows, blocks, ("kv",) * len(blocks), carry)
        carry, waiting = result[:3], ()
        if step == 1:
            rows = result[3:]
        ahead, behind = following
    parts = attend(rows, (ahead, behind), ("k", "v"), carry, parts=low)
    parts = [parts[0]] + [
        lax.ppermute(parts[d], "lo", [(i, (i - d) % low) for i in range(low)])
        for d in range(1, low)
    ]
    return parts, held


def extended(cells, axes, width):
    count = math.prod(lax.axis_size(a) for a in axes)
    ends = count - 1
    head = cells[:, :width]
    tail = cells[:, cells.shape[1] - width :]
    above = lax.ppermute(tail, axes, [(i, i + 1) for i in range(ends)])
    below = lax.ppermute(head, axes, [(i + 1, i) for i in range(ends)])
    return jnp.concatenate([above, cells, below], axis=1)


def window_attend(queries, keys_pad, values_pad, slopes, sink_logits, offset, total_rows):
    query_rows = queries.shape[0]
    block_span = WINDOW // 2
    blocks = query_rows // block_span
    key_heads = keys_pad.shape[1] // HEAD
    group_size = queries.shape[1] // keys_pad.shape[1]
    query_blocks = queries.reshape(blocks, block_span, key_heads, group_size, HEAD)
    key_blocks = keys_pad.reshape(blocks + 4, block_span, key_heads, HEAD)
    value_blocks = values_pad.reshape(blocks + 4, block_span, key_heads, HEAD)
    key_window = jnp.concatenate([key_blocks[s : s + blocks] for s in range(5)], axis=1)
    value_window = jnp.concatenate([value_blocks[s : s + blocks] for s in range(5)], axis=1)
    scores = jnp.einsum(
        "nqkgd,nskd->kgnqs", query_blocks, key_window, preferred_element_type=jnp.float32
    ) * HEAD ** (-0.5)
    query_place = offset + jnp.arange(query_rows, dtype=jnp.int32).reshape(blocks, block_span, 1)
    key_place = (
        offset
        - WINDOW
        + block_span * jnp.arange(blocks, dtype=jnp.int32)[:, None, None]
        + jnp.arange(5 * block_span, dtype=jnp.int32)[None, None, :]
    )
    distance = jnp.abs(key_place - query_place)
    inside = (distance <= WINDOW) & (key_place >= 0) & (key_place < total_rows)
    slope_grid = slopes.reshape(key_heads, group_size, 1, 1, 1)
    sink_grid = sink_logits.reshape(key_heads, group_size, 1, 1)
    scores = jnp.where(inside, scores - slope_grid * distance.astype(jnp.float32), NEGATIVE)
    highest = jnp.maximum(jnp.max(scores, axis=-1), sink_grid)
    raised = jnp.exp(scores - highest[..., None])
    denominator = jnp.sum(raised, axis=-1) + jnp.exp(sink_grid - highest)
    weights = (raised / denominator[..., None]).astype(jnp.bfloat16)
    attended = jnp.einsum(
        "kgnqs,nskd->nqkgd", weights, value_window, preferred_element_type=jnp.float32
    )
    return attended.astype(jnp.bfloat16).reshape(query_rows, -1)


def by_target(rows):
    across = lax.axis_size("x")
    x = lax.axis_index("x")
    core = lax.axis_index("core")
    count = rows.shape[0] // (across * CORES)
    tiles = rows.reshape(across, CORES, count, rows.shape[1])
    tiles = jnp.where(core == 0, tiles, tiles[:, ::-1])
    tiles = lax.dynamic_slice_in_dim(jnp.concatenate([tiles, tiles], axis=0), x, across, axis=0)
    return jnp.swapaxes(tiles, 0, 1).reshape(rows.shape)


def sent_and_summed(here, there):
    across = lax.axis_size("x")
    theirs = lax.ppermute(there, "core", [(0, 1), (1, 0)])
    both = here.astype(jnp.float32) + theirs.astype(jnp.float32)
    tiles = both.astype(jnp.bfloat16).reshape(across, here.shape[0] // across, -1)
    total = tiles[0].astype(jnp.float32)
    for d in range(1, across):
        total = total + lax.ppermute(
            tiles[d], "x", [(i, (i + d) % across) for i in range(across)]
        ).astype(jnp.float32)
    return total


def per_device(
    window_query,
    window_key,
    window_value,
    grid_query,
    grid_key,
    grid_value,
    sink_logit,
    query_gain,
    key_gain,
    window_weights,
    grid_weights,
):
    local_rows = window_query.shape[0]
    planes = ("hi", "lo")
    plane = lax.axis_index("hi") * PLANES + lax.axis_index("lo")
    head_group = lax.axis_index("x") * CORES + lax.axis_index("core")
    offset = plane * local_rows
    total_rows = local_rows * lax.axis_size("hi") * PLANES
    cos, sin = turn_tables(offset, local_rows)
    kv = turn(grid_key, key_gain, cos, sin, grid_value)
    heads = grid_query.shape[1] // HEAD

    def make_queries(after):
        _, given = lax.optimization_barrier((after, grid_query))
        turned = by_target(turn(given, query_gain, cos, sin))
        return jnp.concatenate(
            [turned[:, h * HEAD : (h + 1) * HEAD] for h in range(heads)], axis=0
        )

    parts, (window_query, window_key, window_value) = grid_attend(
        kv, make_queries, (window_query, window_key, window_value)
    )

    local_heads = sink_logit.shape[0]
    head_number = head_group * local_heads + 1 + jnp.arange(local_heads, dtype=jnp.int32)
    slopes = 2.0 ** (-8.0 * head_number.astype(jnp.float32) / QH_A)
    padded = extended(jnp.stack([window_key, window_value]), planes, WINDOW)
    window_out = by_target(
        window_attend(window_query, padded[0], padded[1], slopes, sink_logit, offset, total_rows)
    )
    here, there = project(parts, window_out, window_weights, grid_weights)
    return sent_and_summed(here, there).astype(jnp.bfloat16)


def solution(mesh):
    shape = mesh.shape
    inner = Mesh(
        mesh.devices.reshape(
            shape["grp"], shape["sp"] // PLANES, PLANES, shape["tp"] // CORES, CORES
        ),
        ("grp", "hi", "lo", "x", "core"),
    )
    rows = ("grp", "hi", "lo")
    heads = ("x", "core")

    return jax.shard_map(
        per_device,
        mesh=inner,
        in_specs=(
            P(rows, heads),
            P(rows, heads),
            P(rows, heads),
            P(rows, heads),
            P(rows, heads),
            P(rows, heads),
            P(heads),
            P(),
            P(),
            P(heads, None),
            P(heads, None),
        ),
        out_specs=P(rows + heads, None),
        check_vma=False,
    )
```
